128 devices in a mesh: ep: 64 (over z, y, x), tp: 2 (over core).
Axes of the slice: x: 4, y: 4, z: 4, core: 2. Of those that a mesh axis runs over, the one named last changes fastest.
Arguments:
- stream: bfloat16 [4096, 2048], P('ep', 'tp'), may hold values from -40 to 40
- conv_state: bfloat16 [4096, 3, 2048], P('ep', None, 'tp'), may hold values from -5 to 5
- recur_state: float32 [4096, 2048], P('ep', 'tp'), may hold values from -5 to 5
- mix_gain: float32 [2048], replicated, may hold values from 0.1 to 1.9
- branch_weight: bfloat16 [2048, 2048], P(None, 'tp'), may hold values from -0.125 to 0.125
- gate_weight: bfloat16 [2048, 2048], P(None, 'tp'), may hold values from -0.125 to 0.125
- conv_taps: float32 [4, 2048], P(None, 'tp'), may hold values from -3 to 3
- recur_map: bfloat16 [16, 128, 128], P('tp'), may hold values from -0.5 to 0.5
- input_map: bfloat16 [16, 128, 128], P('tp'), may hold values from -0.5 to 0.5
- decay_logit: float32 [2048], P('tp'), may hold values from -1 to 6
- out_weight: bfloat16 [2048, 2048], P(None, 'tp'), may hold values from -0.125 to 0.125
- moe_gain: float32 [2048], replicated, may hold values from 0.1 to 1.9
- route_ids: int32 [4096, 6], P('ep'), may hold values from 0 to 63, all different within a row; in each aligned block of 64 rows (0 to 63, 64 to 127, ...) at most 18 rows name the same one
- route_weights: float32 [4096, 6], P('ep'), may hold values from 0.2 to 1
- expert_gate: bfloat16 [64, 2048, 512], P('ep', None, 'tp'), may hold values from -0.125 to 0.125
- expert_up: bfloat16 [64, 2048, 512], P('ep', None, 'tp'), may hold values from -0.125 to 0.125
- expert_down: bfloat16 [64, 512, 2048], P('ep', None, 'tp'), may hold values from -0.25 to 0.25
- dense_gate: bfloat16 [2048, 512], P(None, 'tp'), may hold values from -0.125 to 0.125
- dense_up: bfloat16 [2048, 512], P(None, 'tp'), may hold values from -0.125 to 0.125
- dense_down: bfloat16 [512, 2048], P(None, 'tp'), may hold values from -0.25 to 0.25
- dense_scale: float32 [2048], P('tp'), may hold values from 0.1 to 1.9
Outputs:
- result: bfloat16 [4096, 2048], P('ep', 'tp')
- new_state: float32 [4096, 2048], P('ep', 'tp')
- new_conv: bfloat16 [4096, 3, 2048], P('ep', None, 'tp')
The draws below stay inside these ranges and needn't reach their ends.
Inputs may be any that keep to these rules, and one draw needn't show every extreme that they name: `route_ids`: each row names 6 different experts; among the rows of one index of ep no expert is named by more than 18 rows, and in every draw some expert is named by exactly 18 rows of some index.
All inputs are finite; a program needn't handle non-finite values.
Results may differ from the reference program's by a relative error of at most 0.014.
Values may be sent and summed in bfloat16 or wider, within the bound.
A program may use at most 128 MiB of HBM per device.

```python
import math
import jax
import jax.numpy as jnp
import numpy as np
from jax import lax

D = 2048
W = 2048
LBLK = 16
BLK = 128
FFE = 512
FFS = 512
TOP = 6
SEQ_DEV = 64
BATCH = 4096
EXPERTS = 64
CAP = 18
N_EP = 64


def draw_stream(key, part):
    key_cols, key_rows, key_base = jax.random.split(key, 3)
    positions = jnp.arange(D, dtype=jnp.float32) / D
    rough = jnp.exp(jax.random.uniform(key_cols, (D,), jnp.float32, -0.7, 0.7))
    row_scale = jnp.exp(jax.random.uniform(key_rows, (BATCH, 1), jnp.float32, jnp.log(0.5), jnp.log(2.5)))
    column_scale = jnp.exp(jnp.log(3.0) * (positions - 0.5)) * rough
    base = jnp.clip(jax.random.normal(key_base, (BATCH, D), jnp.float32), -4.0, 4.0)
    return (base * column_scale[None, :] * row_scale).astype(jnp.bfloat16)


def levels(rng, shape, cuts, least, high):
    def one(dim, shards_of):
        heights = jax.random.uniform(jax.random.fold_in(jax.random.fold_in(rng, 6), dim), (shards_of,), jnp.float32, least / len(cuts), high / len(cuts))
        return jnp.repeat(jnp.exp(heights), shape[dim] // shards_of).reshape((-1,) + (1,) * (len(shape) - dim - 1))

    level = one(*cuts[0])
    for cut in cuts[1:]:
        level = level * one(*cut)
    return level


def routed_block(key, own, number, rows, count, top, bound, skew):
    order = jax.random.permutation(key, count)
    heavy_load, common = portions_of(count, rows * top, bound, skew, True), portions_of(count, rows * top, bound, skew, False)
    places = jnp.arange(count)

    def named(lengths, offset_by):
        used = int((lengths > 0).sum())
        fixed = max(1, used // 4)
        moved = fixed + (places - fixed + offset_by * (used - fixed)) % max(1, count - fixed)
        return jnp.zeros((count,), jnp.int32).at[order[jnp.where(places < fixed, places, moved)]].set(jnp.asarray(lengths, jnp.int32))

    lengths = jnp.where(number % 4 == 0, named(heavy_load, number // 4), named(common, number - number // 4 - 1))
    mixed = jax.random.permutation(jax.random.fold_in(own, 3), count)
    source_of, taker = mixed[0:count // 2 * 2:2], mixed[1:count // 2 * 2:2]
    slack = jnp.minimum(lengths[source_of] - 1, bound - lengths[taker]) // 2
    slack = jnp.where((source_of == order[0]) | (taker == order[0]) | (lengths[taker] == 0), 0, jnp.maximum(slack, 0))
    moved = jax.random.randint(jax.random.fold_in(own, 4), (count // 2,), 0, 1 << 20) % (slack + 1)
    lengths = lengths.at[source_of].add(-moved).at[taker].add(moved)
    labels = jnp.searchsorted(jnp.cumsum(lengths), jnp.arange(rows * top), side="right").astype(jnp.int32)
    listing = labels.reshape(top, rows).T
    listing = listing[jax.random.permutation(jax.random.fold_in(own, 1), rows)]
    offset_by = jax.random.randint(jax.random.fold_in(own, 2), (rows, 1), 0, top)
    return jnp.take_along_axis(listing, (jnp.arange(top)[None, :] + offset_by) % top, axis=1)


def portions_of(amount, total, limit, lean, full):
    portions = [(1 << 20) // math.isqrt(grade ** lean) + 1 for grade in range(1, amount + 1)]
    largest = limit if full else min(limit, max(-(-total // amount), total * portions[0] // sum(portions)))
    least = 1 if total - largest >= amount - 1 else 0
    counts, surplus = [largest] + [least] * (amount - 1), total - largest - least * (amount - 1)
    while surplus > 0:
        free = [i for i in range(1, amount) if counts[i] < largest] or [i for i in range(1, amount) if counts[i] < limit]
        mass, remaining = sum([portions[i] for i in free]), surplus
        for i in free:
            addition = min(limit - counts[i], max(1, remaining * portions[i] // mass), surplus)
            counts[i] = counts[i] + addition
            surplus = surplus - addition
    return np.array(counts)


def noise(stream_key, shape, spread, limit, cuts=(), kind=jnp.bfloat16):
    array = spread * jax.random.normal(stream_key, shape, jnp.float32)
    if cuts:
        array = array * levels(stream_key, shape, cuts, -0.22, 0.18)
    return jnp.clip(array, -limit, limit).astype(kind)


def setup_inputs(seed: int = 0) -> dict:
    arg_keys = jax.random.split(jax.random.key(seed), 22)
    stream = draw_stream(jax.random.fold_in(arg_keys[21], 71), 0)
    conv_state = noise(arg_keys[1], (BATCH, 3, W), 1.0, 5.0, ((0, 64), (2, 2)))
    recur_state = noise(arg_keys[2], (BATCH, W), 1.0, 5.0, ((0, 64), (1, 2)), jnp.float32)
    mix_gain = jnp.clip(1.0 + 0.18 * jax.random.normal(arg_keys[3], (D,), jnp.float32), 0.1, 1.9)
    branch_weight = noise(arg_keys[4], (D, W), D ** -0.5, 0.125, ((1, 2),))
    gate_weight = noise(arg_keys[5], (D, W), D ** -0.5, 0.125, ((1, 2),))
    conv_taps = noise(arg_keys[6], (4, W), 0.5, 3.0, ((1, 2),), jnp.float32)
    recur_map = noise(arg_keys[7], (LBLK, BLK, BLK), BLK ** -0.5, 0.5, ((0, 2),))
    input_map = noise(arg_keys[8], (LBLK, BLK, BLK), BLK ** -0.5, 0.5, ((0, 2),))
    decay_logit = jnp.clip(-1.0 + 7.0 * jax.random.uniform(arg_keys[9], (W,), jnp.float32) ** levels(arg_keys[9], (W,), ((0, 2),), -0.2, 0.2), -1.0, 6.0)
    out_weight = noise(arg_keys[10], (W, D), W ** -0.5, 0.125, ((1, 2),))
    moe_gain = jnp.clip(1.0 + 0.18 * jax.random.normal(arg_keys[11], (D,), jnp.float32), 0.1, 1.9)
    route_ids_keys = jax.random.split(jax.random.fold_in(arg_keys[12], 1), BATCH // SEQ_DEV)
    route_ids_turns = jax.random.permutation(jax.random.fold_in(arg_keys[12], 3), BATCH // SEQ_DEV)
    route_ids = jax.vmap(lambda own, number: routed_block(jax.random.fold_in(arg_keys[12], 2), own, number, SEQ_DEV, EXPERTS, TOP, CAP, 1))(route_ids_keys, route_ids_turns).reshape((BATCH, TOP))
    route_weights = jnp.clip(0.2 + 0.8 * jax.random.uniform(arg_keys[13], (BATCH, TOP), jnp.float32) ** levels(arg_keys[13], (BATCH, TOP), ((0, 64),), -0.2, 0.2), 0.2, 1.0)
    expert_gate = noise(arg_keys[14], (EXPERTS, D, FFE), D ** -0.5, 0.125, ((0, 64), (2, 2)))
    expert_up = noise(arg_keys[15], (EXPERTS, D, FFE), D ** -0.5, 0.125, ((0, 64), (2, 2)))
    expert_down = noise(arg_keys[16], (EXPERTS, FFE, D), FFE ** -0.5, 0.25, ((0, 64), (2, 2)))
    dense_gate = noise(arg_keys[17], (D, FFS), D ** -0.5, 0.125, ((1, 2),))
    dense_up = noise(arg_keys[18], (D, FFS), D ** -0.5, 0.125, ((1, 2),))
    dense_down = noise(arg_keys[19], (FFS, D), FFS ** -0.5, 0.25, ((1, 2),))
    dense_scale = jnp.clip(1.0 + 0.18 * jax.random.normal(arg_keys[20], (D,), jnp.float32), 0.1, 1.9)
    return dict(stream=stream, conv_state=conv_state, recur_state=recur_state, mix_gain=mix_gain, branch_weight=branch_weight, gate_weight=gate_weight, conv_taps=conv_taps, recur_map=recur_map, input_map=input_map, decay_logit=decay_logit, out_weight=out_weight, moe_gain=moe_gain, route_ids=route_ids, route_weights=route_weights, expert_gate=expert_gate, expert_up=expert_up, expert_down=expert_down, dense_gate=dense_gate, dense_up=dense_up, dense_down=dense_down, dense_scale=dense_scale)


def layer_normed(values, gain_vec):
    widened = values.astype(jnp.float32)
    row_mean = lax.optimization_barrier(jnp.mean(widened, axis=-1, keepdims=True))
    row_var = lax.optimization_barrier(jnp.mean(widened * widened, axis=-1, keepdims=True)) - row_mean * row_mean
    return ((widened - row_mean) * lax.rsqrt(row_var + 1e-05) * gain_vec).astype(jnp.bfloat16)

def gated_rows(inputs, w_gate, w_up, w_down):
    gate_sum = jnp.dot(inputs, w_gate, preferred_element_type=jnp.float32)
    up_sum = jnp.dot(inputs, w_up, preferred_element_type=jnp.float32)
    hidden = (jax.nn.silu(gate_sum) * up_sum).astype(jnp.bfloat16)
    return jnp.dot(hidden, w_down, preferred_element_type=jnp.float32).astype(jnp.bfloat16)

def reference(stream, conv_state, recur_state, mix_gain, branch_weight, gate_weight, conv_taps, recur_map, input_map, decay_logit, out_weight, moe_gain, route_ids, route_weights, expert_gate, expert_up, expert_down, dense_gate, dense_up, dense_down, dense_scale):
    normed = layer_normed(stream, mix_gain)
    branch_in = jnp.dot(normed, branch_weight, preferred_element_type=jnp.float32).astype(jnp.bfloat16)
    gate_pre = jnp.dot(normed, gate_weight, preferred_element_type=jnp.float32).astype(jnp.bfloat16)
    conv_sum = branch_in.astype(jnp.float32) * conv_taps[3]
    for offset in range(3):
        conv_sum = conv_sum + conv_state[:, offset].astype(jnp.float32) * conv_taps[offset]
    conv_out = conv_sum.astype(jnp.bfloat16)
    new_conv = jnp.concatenate([conv_state[:, 1:], branch_in[:, None]], axis=1)
    grouped = conv_out.astype(jnp.float32).reshape(BATCH, LBLK, BLK)
    recur_gate = jax.nn.sigmoid(jnp.einsum('nbc,bcd->nbd', grouped, recur_map.astype(jnp.float32))).reshape(BATCH, W)
    input_gate = jax.nn.sigmoid(jnp.einsum('nbc,bcd->nbd', grouped, input_map.astype(jnp.float32))).reshape(BATCH, W)
    log_decay = -8.0 * recur_gate * jax.nn.softplus(-decay_logit)
    driven = jnp.sqrt(-jnp.expm1(2.0 * log_decay)) * (input_gate * conv_out.astype(jnp.float32))
    new_state = jnp.exp(log_decay) * recur_state + driven
    mixer_in = (jax.nn.gelu(gate_pre.astype(jnp.float32)) * new_state).astype(jnp.bfloat16)
    mixer_out = jnp.dot(mixer_in, out_weight, preferred_element_type=jnp.float32).astype(jnp.bfloat16)
    resid = (stream.astype(jnp.float32) + mixer_out.astype(jnp.float32)).astype(jnp.bfloat16)
    normed_two = layer_normed(resid, moe_gain)
    flat_ids = route_ids.reshape(N_EP, SEQ_DEV * TOP)
    one_hot = (flat_ids[:, :, None] == jnp.arange(EXPERTS, dtype=jnp.int32)[None, None, :]).astype(jnp.int32)
    slot_rank = lax.optimization_barrier(jnp.sum(one_hot * (jnp.cumsum(one_hot, axis=1) - 1), axis=2))
    block_ids = jnp.arange(N_EP, dtype=jnp.int32)[:, None]
    column = (block_ids * CAP + slot_rank).reshape(-1).astype(jnp.int32)
    token_ids = (jnp.arange(BATCH * TOP, dtype=jnp.int32) // TOP).astype(jnp.int32)
    row_token = jnp.full((EXPERTS, N_EP * CAP), BATCH, jnp.int32).at[route_ids.reshape(-1), column].set(token_ids)
    padded = jnp.concatenate([normed_two, jnp.zeros((1, D), jnp.bfloat16)], axis=0)

    def one_expert(packed):
        rows_taken, w_gate, w_up, w_down = packed
        return gated_rows(padded[rows_taken], w_gate, w_up, w_down)
    outputs = lax.map(one_expert, (row_token, expert_gate, expert_up, expert_down))
    picked = outputs[route_ids.reshape(-1), column].reshape(BATCH, TOP, D)
    routed = lax.optimization_barrier(jnp.sum(picked.astype(jnp.float32) * route_weights[:, :, None], axis=1))
    dense_out = gated_rows(normed_two, dense_gate, dense_up, dense_down)
    result = (resid.astype(jnp.float32) + routed + dense_scale * dense_out.astype(jnp.float32)).astype(jnp.bfloat16)
    return (result, new_state, new_conv)
```

```python
import jax
import jax.numpy as jnp
from jax import lax
from jax.experimental import pallas as pl
from jax.experimental.pallas import tpu as pltpu
from jax.sharding import PartitionSpec as P

BF = jnp.bfloat16
F32 = jnp.float32
MESH = pl.DeviceIdType.MESH

ROWS = 64
META = 8
BLOCK = ROWS + META
CUT = 40
HALF = 1024
LANES = ((0, 384), (384, 384), (768, 256))
ORDERS = ((0, 1, 2), (1, 2, 0), (2, 0, 1))
STRIDE = (16, 4, 1)
N_SEM = 256


def gathered_index(order, i, j):
    return (j, i) if order == 2 else (i, j)


def canonical(order, d, h):
    part = slice(None) if h is None else pl.ds(2 * h, 2)
    if order == 0:
        return (part, slice(None), d)
    if order == 1:
        return (d, part, slice(None))
    return (part, d, slice(None))


def power_of_two(exponent):
    value = jnp.ones(exponent.shape, F32)
    for bit in range(6):
        value = value * jnp.where((exponent >> bit) & 1 == 1, F32(2.0 ** (2**bit)), F32(1.0))
    return value


def dot(a, b):
    return jnp.dot(a, b, preferred_element_type=F32)


def dot_t(a, b):
    return lax.dot_general(a, b, (((0,), (0,)), ((), ())), preferred_element_type=F32)


def moe_kernel(
    n2, resid, ids_ref, wts_ref, scale_ref, eg, eu, ed, dg, du, dd,
    out,
    w_eg, w_eu, w_ed, w_dg, w_du, w_dd,
    ag0, ag1, ag2, cm0, cm1, cm2, ce0, ce1, ce2, fm0, fm1, fm2, fe0, fe1, fe2,
    xm, xe0, xe1, xe2, xx, hid, ym, yx, ye0, ye1, ye2,
    rm0, rm1, rm2, re0, re1, re2, gm0, gm1, gm2, ge0, ge1, ge2,
    pt0, pt1, pt2, sb0, sb1, sb2, rb0, rb1, rb2,
    pick_m, pick_e, comb_m, comb_e, dh, dense,
    ss, rs, ws,
):
    ag, cm, ce, fm, fe = (ag0, ag1, ag2), (cm0, cm1, cm2), (ce0, ce1, ce2), (fm0, fm1, fm2), (fe0, fe1, fe2)
    xe, ye, rm, re = (xe0, xe1, xe2), (ye0, ye1, ye2), (rm0, rm1, rm2), (re0, re1, re2)
    gm, ge, pt, sb, rb = (gm0, gm1, gm2), (ge0, ge1, ge2), (pt0, pt1, pt2), (sb0, sb1, sb2), (rb0, rb1, rb2)
    ep = lax.axis_index("ep")
    core = lax.axis_index("tp")
    coord = (ep // 16, (ep // 4) % 4, ep % 4)

    def along(axis, step):
        c = coord[axis]
        return ep + ((c + step) % 4 - c) * STRIDE[axis]

    next_dev = tuple((along(a, 1), core) for a in range(3))
    prev_dev = tuple((along(a, 3), core) for a in range(3))
    partner = (ep, 1 - core)

    barrier = pltpu.get_barrier_semaphore()
    for dev in (*next_dev, *prev_dev, partner):
        pl.semaphore_signal(barrier, inc=1, device_id=dev, device_id_type=MESH)

    loads = []

    def load(src, dst):
        copy = pltpu.make_async_copy(src, dst, ws.at[len(loads)])
        copy.start()
        loads.append(copy)

    own = pl.multiple_of(core * HALF, HALF)
    other = pl.multiple_of((1 - core) * HALF, HALF)
    own_h = pl.multiple_of(core * 256, 256)
    other_h = pl.multiple_of((1 - core) * 256, 256)
    for src, dst in ((dg, w_dg), (du, w_du)):
        load(src.at[pl.ds(own, HALF)], dst.at[0])
        load(src.at[pl.ds(other, HALF)], dst.at[1])
    load(dd.at[pl.ds(own_h, 256)], w_dd.at[0])
    load(dd.at[pl.ds(other_h, 256)], w_dd.at[1])
    for src, dst in ((eg, w_eg), (eu, w_eu)):
        load(src.at[0, pl.ds(own, HALF)], dst.at[0])
        load(src.at[0, pl.ds(other, HALF)], dst.at[1])
    load(ed.at[0, pl.ds(own_h, 256)], w_ed.at[0])
    load(ed.at[0, pl.ds(other_h, 256)], w_ed.at[1])

    used = [0]

    def remote(src, dst, dev):
        k = used[0]
        used[0] += 1
        return pltpu.make_async_remote_copy(
            src_ref=src, dst_ref=dst, send_sem=ss.at[k], recv_sem=rs.at[k], device_id=dev, device_id_type=MESH
        )

    sent = []

    def go(copy):
        copy.start()
        sent.append(copy)
        return copy

    lane = lax.broadcasted_iota(jnp.int32, (64, 128), 1)
    row = lax.broadcasted_iota(jnp.int32, (64, 128), 0)
    twice = (lane % 64 == row).astype(BF)
    ids_t = dot_t(ids_ref[...].astype(F32).astype(BF), twice)
    wts_t = dot_t(wts_ref[...].astype(BF), twice)
    experts = row.astype(F32)
    chosen = jnp.zeros((64, 128), F32)
    for k in range(6):
        chosen = chosen + jnp.where(ids_t[k : k + 1] == experts, F32(1.0), F32(0.0))
    earlier = ((lane % 64 > row)).astype(BF)
    rank = dot(chosen[:, :64].astype(BF), earlier)
    code = (rank + 32.0) * power_of_two(row)
    codes = [
        jnp.sum(jnp.where(ids_t[k : k + 1] == experts, code, F32(0.0)), axis=0, keepdims=True) for k in range(6)
    ]
    zeros2 = jnp.zeros((2, 128), F32)
    code8 = jnp.concatenate([*codes, zeros2], axis=0).astype(BF)
    wts8 = jnp.concatenate([wts_t, zeros2], axis=0).astype(BF)
    for o, (l0, w) in enumerate(LANES):
        ag[o][0, 0, 0:ROWS, :] = n2[0, :, l0 : l0 + w]
        ag[o][0, 0, ROWS:BLOCK, 0:128] = code8
        ag[o][0, 0, ROWS:BLOCK, 128:256] = wts8
        if w > 256:
            ag[o][0, 0, ROWS:BLOCK, 256:w] = jnp.zeros((META, w - 256), BF)

    pl.semaphore_wait(barrier, 7)

    def block(o, i, j, part=None):
        u, v = gathered_index(o, i, j)
        return ag[o].at[u, v] if part is None else ag[o].at[u, v, part]

    top, low = pl.ds(0, CUT), pl.ds(CUT, BLOCK - CUT)
    t1, t2, u1, u2 = {}, {}, {}, {}
    for o in range(3):
        a1, a2, _ = ORDERS[o]
        t1[o] = (
            go(remote(block(o, 0, 0), block(o, 3, 0), next_dev[a1])),
            go(remote(block(o, 0, 0), block(o, 1, 0), prev_dev[a1])),
        )

    def spread(o, i):
        a2 = ORDERS[o][1]
        u1[o, i] = (
            go(remote(block(o, i, 0), block(o, i, 3), next_dev[a2])),
            go(remote(block(o, i, 0), block(o, i, 1), prev_dev[a2])),
        )

    def relay(o, i):
        a2 = ORDERS[o][1]
        u1[o, i][0].wait_recv()
        u1[o, i][1].wait_recv()
        u2[o, i] = (
            go(remote(block(o, i, 3, top), block(o, i, 2, top), next_dev[a2])),
            go(remote(block(o, i, 1, low), block(o, i, 2, low), prev_dev[a2])),
        )

    for o in range(3):
        spread(o, 0)

    for h in range(2):
        for o in range(3):
            comb_m[o, h] = jnp.zeros((512, 512), BF)
            comb_e[o, h] = jnp.zeros((64, 512), BF)
    for b in range(2):
        pick_m[b] = jnp.zeros((512, 512), BF)

    for o in range(3):
        a1 = ORDERS[o][0]
        t1[o][0].wait_recv()
        t1[o][1].wait_recv()
        t2[o] = (
            go(remote(block(o, 3, 0, top), block(o, 2, 0, top), next_dev[a1])),
            go(remote(block(o, 1, 0, low), block(o, 2, 0, low), prev_dev[a1])),
        )
        spread(o, 3)
        spread(o, 1)
    for o in range(3):
        relay(o, 0)
    for o in range(3):
        t2[o][0].wait_recv()
        t2[o][1].wait_recv()
        spread(o, 2)
    for o in range(3):
        relay(o, 3)
        relay(o, 1)

    for copy in loads[:6]:
        copy.wait()
    n_own, n_other = n2[0], n2[1]
    d_gate = dot(n_own, w_dg[0]) + dot(n_other, w_dg[1])
    d_up = dot(n_own, w_du[0]) + dot(n_other, w_du[1])
    dh[0] = (jax.nn.silu(d_gate) * d_up).astype(BF)
    dh_copy = go(remote(dh.at[0], dh.at[1], partner))

    for o in range(3):
        relay(o, 2)
    dh_copy.wait_recv()
    dense[...] = (dot(dh[0], w_dd[0]) + dot(dh[1], w_dd[1])).astype(BF).astype(F32)

    lane128 = lax.broadcasted_iota(jnp.int32, (16, 128), 1)
    rank16 = lax.broadcasted_iota(jnp.int32, (16, 128), 0).astype(F32) + 32.0
    lane512 = lax.broadcasted_iota(jnp.int32, (16, 512), 1)
    row512 = lax.broadcasted_iota(jnp.int32, (16, 512), 0)
    extra_rank = (row512 % 2).astype(F32) + 48.0
    extra_own = lane512 // 64 == row512 // 2
    first_half = lax.broadcasted_iota(jnp.int32, (8, 128), 1) < 64
    arrived = {}

    def pick(o, h, buf):
        l0, w = LANES[o]
        a3 = ORDERS[o][2]
        code, weight = [], []
        for p in range(4):
            left = (2 * h + (2 * p) // 4, (2 * p) % 4)
            right = (2 * h + (2 * p + 1) // 4, (2 * p + 1) % 4)
            for into, at in ((code, 0), (weight, 128)):
                a = ag[o][left[0], left[1], ROWS:BLOCK, at : at + 128].astype(F32)
                b = ag[o][right[0], right[1], ROWS:BLOCK, at : at + 128].astype(F32)
                into.append(jnp.where(first_half, a, b))
        code = jnp.concatenate(code, axis=1)
        weight = jnp.concatenate(weight, axis=1)
        for d in range(4):
            scale = power_of_two(jnp.full((8, 512), along(a3, d), jnp.int32))
            mine = (code >= 32.0 * scale) & (code < 64.0 * scale)
            ranks = jnp.sum(jnp.where(mine, code, F32(0.0)), axis=0, keepdims=True)
            weights = jnp.sum(jnp.where(mine, weight, F32(0.0)), axis=0, keepdims=True)
            one = scale[0:1, 0:128]
            for s in range(8):
                lo = 128 * (s // 2)
                hit = (ranks[:, lo : lo + 128] == rank16 * one) & ((lane128 // 64) == s % 2)
                at = slice(128 * d + 16 * s, 128 * d + 16 * s + 16)
                pick_m[buf, at, lo : lo + 128] = jnp.where(hit, F32(1.0), F32(0.0)).astype(BF)
                comb_m[o, h, at, lo : lo + 128] = jnp.where(hit, weights[:, lo : lo + 128], F32(0.0)).astype(BF)
            hit = (ranks == extra_rank * scale[0:1]) & extra_own
            pick_e[buf, 16 * d : 16 * d + 16] = jnp.where(hit, F32(1.0), F32(0.0)).astype(BF)
            comb_e[o, h, 16 * d : 16 * d + 16] = jnp.where(hit, weights, F32(0.0)).astype(BF)
        rows = ag[o][2 * h : 2 * h + 2, :, 0:ROWS, :].reshape(512, w)
        main = dot(pick_m[buf], rows).astype(BF)
        extra = dot(pick_e[buf], rows).astype(BF)
        for d in range(4):
            m = main[128 * d : 128 * d + 128].reshape(2, 4, 16, w)
            e = extra[16 * d : 16 * d + 16]
            if d == 0:
                xm[(0, *canonical(o, 0, h), slice(None), pl.ds(l0, w))] = m
                xe[o][0, 0, h] = e
            else:
                cm[o][d - 1, h] = m
                ce[o][d - 1, h] = e
        ahead, behind = next_dev[a3], prev_dev[a3]
        far = ahead if h == 0 else behind
        into = lambda d: xm.at[(0, *canonical(o, d, h), slice(None), pl.ds(l0, w))]
        arrived[o, 2, h] = (
            go(remote(cm[o].at[1, h], fm[o].at[h], far)),
            go(remote(ce[o].at[1, h], fe[o].at[h], far)),
        )
        arrived[o, 3, h] = (
            go(remote(cm[o].at[0, h], into(3), ahead)),
            go(remote(ce[o].at[0, h], xe[o].at[0, 3, h], ahead)),
        )
        arrived[o, 1, h] = (
            go(remote(cm[o].at[2, h], into(1), behind)),
            go(remote(ce[o].at[2, h], xe[o].at[0, 1, h], behind)),
        )

    for o in range(3):
        for i in range(4):
            u2[o, i][0].wait_recv()
            u2[o, i][1].wait_recv()
        for h in range(2):
            pick(o, h, h)

    crossed = []

    def across(o, d):
        l0, w = LANES[o]
        at = (*canonical(o, d, None), slice(None), pl.ds(l0, w))
        crossed.append(go(remote(xm.at[(0, *at)], xm.at[(1, *at)], partner)))
        crossed.append(go(remote(xe[o].at[0, d], xe[o].at[1, d], partner)))

    for o in range(3):
        across(o, 0)
    for o in range(3):
        l0, w = LANES[o]
        a3 = ORDERS[o][2]
        for h in range(2):
            for copy in arrived[o, 2, h]:
                copy.wait_recv()
            far = next_dev[a3] if h == 0 else prev_dev[a3]
            arrived[o, 4, h] = (
                go(remote(fm[o].at[h], xm.at[(0, *canonical(o, 2, h), slice(None), pl.ds(l0, w))], far)),
                go(remote(fe[o].at[h], xe[o].at[0, 2, h], far)),
            )
    for d in (3, 1):
        for o in range(3):
            for h in range(2):
                for copy in arrived[o, d, h]:
                    copy.wait_recv()
            across(o, d)
    for o in range(3):
        for h in range(2):
            for copy in arrived[o, 4, h]:
                copy.wait_recv()
        across(o, 2)
    for copy in loads[6:]:
        copy.wait()
    for copy in crossed:
        copy.wait_recv()

    r128 = lax.broadcasted_iota(jnp.int32, (128, 128), 0)
    c128 = lax.broadcasted_iota(jnp.int32, (128, 128), 1)
    dz, dy, dx, bit = r128 // 32, (r128 // 8) % 4, (r128 // 2) % 4, r128 % 2
    turn = {
        0: (c128 == (dx * 16 + dz * 4 + dy) * 2 + bit).astype(BF),
        2: (c128 == (dy * 16 + dz * 4 + dx) * 2 + bit).astype(BF),
    }
    for c in range(2):
        for o, (l0, w) in enumerate(LANES):
            rows = xe[o][c].reshape(128, w)
            xx[c, :, l0 : l0 + w] = rows if o == 1 else dot(turn[o], rows).astype(BF)

    hid_copies = []
    for b in range(5):
        if b < 4:
            x_own, x_other = xm[0, b].reshape(256, HALF), xm[1, b].reshape(256, HALF)
        else:
            x_own, x_other = xx[0], xx[1]
        at = slice(256 * b, 256 * b + x_own.shape[0])
        gate = dot(x_own, w_eg[0]) + dot(x_other, w_eg[1])
        up = dot(x_own, w_eu[0]) + dot(x_other, w_eu[1])
        hid[0, at] = (jax.nn.silu(gate) * up).astype(BF)
        span = pl.ds(256 * b, x_own.shape[0])
        hid_copies.append(go(remote(hid.at[0, span], hid.at[1, span], partner)))
    for b in range(5):
        hid_copies[b].wait_recv()
        size = 256 if b < 4 else 128
        at = slice(256 * b, 256 * b + size)
        y = (dot(hid[0, at], w_ed[0]) + dot(hid[1, at], w_ed[1])).astype(BF)
        if b < 4:
            ym[b] = y.reshape(4, 4, 16, HALF)
        else:
            yx[...] = y
    for o, (l0, w) in enumerate(LANES):
        rows = yx[:, l0 : l0 + w]
        rows = rows if o == 1 else dot_t(turn[o], rows).astype(BF)
        ye[o][...] = rows.reshape(4, 2, 16, w)

    back = {}
    for o, (l0, w) in enumerate(LANES):
        a3 = ORDERS[o][2]
        ahead, behind = next_dev[a3], prev_dev[a3]
        part = lambda d, h: ym.at[(*canonical(o, d, h), slice(None), pl.ds(l0, w))]
        for h in range(2):
            far = ahead if h == 0 else behind
            back[o, 2, h] = (
                go(remote(part(2, h), gm[o].at[h], far)),
                go(remote(ye[o].at[2, h], ge[o].at[h], far)),
            )
        for h in range(2):
            back[o, 3, h] = (
                go(remote(part(1, h), rm[o].at[h, 3], ahead)),
                go(remote(ye[o].at[1, h], re[o].at[h, 3], ahead)),
            )
            back[o, 1, h] = (
                go(remote(part(3, h), rm[o].at[h, 1], behind)),
                go(remote(ye[o].at[3, h], re[o].at[h, 1], behind)),
            )
    for o, (l0, w) in enumerate(LANES):
        for h in range(2):
            rm[o][h, 0] = ym[(*canonical(o, 0, h), slice(None), pl.ds(l0, w))]
            re[o][h, 0] = ye[o][0, h]
    for o in range(3):
        a3 = ORDERS[o][2]
        for h in range(2):
            for copy in back[o, 2, h]:
                copy.wait_recv()
            far = next_dev[a3] if h == 0 else prev_dev[a3]
            back[o, 4, h] = (
                go(remote(gm[o].at[h], rm[o].at[h, 2], far)),
                go(remote(ge[o].at[h], re[o].at[h, 2], far)),
            )
    for o, (l0, w) in enumerate(LANES):
        for h in range(2):
            for d in (3, 1, 4):
                for copy in back[o, d, h]:
                    copy.wait_recv()
            part = dot_t(comb_m[o, h], rm[o][h].reshape(512, w)) + dot_t(comb_e[o, h], re[o][h].reshape(64, w))
            pt[o][2 * h : 2 * h + 2] = part.reshape(2, 4, ROWS, w)

    up32, low32 = slice(0, 32), slice(32, 64)
    stage_a, stage_b = {}, {}

    def at_sum(o, i, j):
        return (j, i) if o == 2 else (i, j)

    def start_far(o, n, axis, src):
        sb[o][n, 0] = pt[o][src].astype(BF)
        stage_a[o, n] = (
            go(remote(sb[o].at[n, 0, pl.ds(0, 32)], rb[o].at[n, 0, pl.ds(0, 32)], prev_dev[axis])),
            go(remote(sb[o].at[n, 0, pl.ds(32, 32)], rb[o].at[n, 0, pl.ds(32, 32)], next_dev[axis])),
        )

    def start_near(o, n, axis, third, first):
        stage_a[o, n][0].wait_recv()
        stage_a[o, n][1].wait_recv()
        sb[o][n, 1, 0:32] = (pt[o][(*third, up32)] + rb[o][n, 0, 0:32].astype(F32)).astype(BF)
        sb[o][n, 1, 32:64] = pt[o][(*third, low32)].astype(BF)
        sb[o][n, 2, 0:32] = pt[o][(*first, up32)].astype(BF)
        sb[o][n, 2, 32:64] = (pt[o][(*first, low32)] + rb[o][n, 0, 32:64].astype(F32)).astype(BF)
        stage_b[o, n] = (
            go(remote(sb[o].at[n, 1], rb[o].at[n, 1], prev_dev[axis])),
            go(remote(sb[o].at[n, 2], rb[o].at[n, 2], next_dev[axis])),
        )

    def finish(o, n, home):
        stage_b[o, n][0].wait_recv()
        stage_b[o, n][1].wait_recv()
        pt[o][home] = pt[o][home] + rb[o][n, 1].astype(F32) + rb[o][n, 2].astype(F32)

    for i in (2, 1, 3, 0):
        for o in range(3):
            start_far(o, i, ORDERS[o][1], at_sum(o, i, 2))
    for i in (2, 1, 3, 0):
        for o in range(3):
            start_near(o, i, ORDERS[o][1], at_sum(o, i, 3), at_sum(o, i, 1))
    for i in (2, 1, 3, 0):
        for o in range(3):
            finish(o, i, at_sum(o, i, 0))
            if i == 2:
                start_far(o, 4, ORDERS[o][0], at_sum(o, 2, 0))
            if i == 3:
                start_near(o, 4, ORDERS[o][0], at_sum(o, 3, 0), at_sum(o, 1, 0))
    for o, (l0, w) in enumerate(LANES):
        finish(o, 4, (0, 0))
        at = slice(l0, l0 + w)
        total = resid[:, at].astype(F32) + pt[o][0, 0] + scale_ref[:, at] * dense[:, at]
        out[:, at] = total.astype(BF)
    for copy in sent:
        copy.wait_send()


def moe(n2, resid, ids, wts, scale, eg, eu, ed, dg, du, dd):
    vmem = pl.BlockSpec(memory_space=pltpu.VMEM)
    anyspace = pl.BlockSpec(memory_space=pl.ANY)
    widths = [w for _, w in LANES]
    per = lambda f, dt=BF: [pltpu.VMEM(f(w), dt) for w in widths]
    scratch = [
        pltpu.VMEM((2, HALF, 256), BF), pltpu.VMEM((2, HALF, 256), BF), pltpu.VMEM((2, 256, HALF), BF),
        pltpu.VMEM((2, HALF, 256), BF), pltpu.VMEM((2, HALF, 256), BF), pltpu.VMEM((2, 256, HALF), BF),
        *per(lambda w: (4, 4, BLOCK, w)),
        *per(lambda w: (3, 2, 2, 4, 16, w)),
        *per(lambda w: (3, 2, 16, w)),
        *per(lambda w: (2, 2, 4, 16, w)),
        *per(lambda w: (2, 16, w)),
        pltpu.VMEM((2, 4, 4, 4, 16, HALF), BF),
        *per(lambda w: (2, 4, 2, 16, w)),
        pltpu.VMEM((2, 128, HALF), BF),
        pltpu.VMEM((2, 1152, 256), BF),
        pltpu.VMEM((4, 4, 4, 16, HALF), BF),
        pltpu.VMEM((128, HALF), BF),
        *per(lambda w: (4, 2, 16, w)),
        *per(lambda w: (2, 4, 2, 4, 16, w)),
        *per(lambda w: (2, 4, 16, w)),
        *per(lambda w: (2, 2, 4, 16, w)),
        *per(lambda w: (2, 16, w)),
        *per(lambda w: (4, 4, ROWS, w), F32),
        *per(lambda w: (5, 3, ROWS, w)),
        *per(lambda w: (5, 3, ROWS, w)),
        pltpu.VMEM((2, 512, 512), BF), pltpu.VMEM((2, 64, 512), BF),
        pltpu.VMEM((3, 2, 512, 512), BF), pltpu.VMEM((3, 2, 64, 512), BF),
        pltpu.VMEM((2, ROWS, 256), BF), pltpu.VMEM((ROWS, HALF), F32),
        pltpu.SemaphoreType.DMA((N_SEM,)), pltpu.SemaphoreType.DMA((N_SEM,)), pltpu.SemaphoreType.DMA((12,)),
    ]
    return pl.pallas_call(
        moe_kernel,
        out_shape=jax.ShapeDtypeStruct((ROWS, HALF), BF),
        in_specs=[vmem] * 5 + [anyspace] * 6,
        out_specs=vmem,
        scratch_shapes=scratch,
        compiler_params=pltpu.CompilerParams(
            collective_id=0, has_side_effects=True, vmem_limit_bytes=60 * 1024 * 1024
        ),
        name="moe",
    )(n2, resid, ids, wts, scale, eg, eu, ed, dg, du, dd)


def gathered_copies(shard, axis, dim):
    return lax.all_gather(shard, axis, axis=dim, tiled=True)


def normalize(part_rows, gain_vec):
    whole_rows = gathered_copies(part_rows, "tp", 1).astype(jnp.float32)
    row_mean = jnp.mean(whole_rows, axis=1, keepdims=True)
    row_var = jnp.mean(whole_rows * whole_rows, axis=1, keepdims=True) - row_mean * row_mean
    return ((whole_rows - row_mean) * lax.rsqrt(row_var + 1e-05) * gain_vec).astype(jnp.bfloat16)


def per_device(
    stream, conv_state, recur_state, mix_gain, branch_weight, gate_weight, conv_taps, recur_map, input_map,
    decay_logit, out_weight, moe_gain, route_ids, route_weights, expert_gate, expert_up, expert_down,
    dense_gate, dense_up, dense_down, dense_scale,
):
    seq_count = stream.shape[0]
    normed = normalize(stream, mix_gain)
    branch_in = jnp.dot(normed, branch_weight, preferred_element_type=jnp.float32).astype(jnp.bfloat16)
    gate_pre = jnp.dot(normed, gate_weight, preferred_element_type=jnp.float32).astype(jnp.bfloat16)
    conv_sum = branch_in.astype(jnp.float32) * conv_taps[3]
    for offset in range(3):
        conv_sum = conv_sum + conv_state[:, offset].astype(jnp.float32) * conv_taps[offset]
    conv_out = conv_sum.astype(jnp.bfloat16)
    new_conv = jnp.concatenate([conv_state[:, 1:], branch_in[:, None]], axis=1)
    grouped = conv_out.reshape(seq_count, recur_map.shape[0], recur_map.shape[1])
    recur_gate = jax.nn.sigmoid(
        jnp.einsum("nbc,bcd->nbd", grouped, recur_map, preferred_element_type=jnp.float32)
    ).reshape(seq_count, -1)
    input_gate = jax.nn.sigmoid(
        jnp.einsum("nbc,bcd->nbd", grouped, input_map, preferred_element_type=jnp.float32)
    ).reshape(seq_count, -1)
    log_decay = -8.0 * recur_gate * jax.nn.softplus(-decay_logit)
    driven = jnp.sqrt(-jnp.expm1(2.0 * log_decay)) * (input_gate * conv_out.astype(jnp.float32))
    new_state = jnp.exp(log_decay) * recur_state + driven
    mixer_in = (jax.nn.gelu(gate_pre.astype(jnp.float32)) * new_state).astype(jnp.bfloat16)
    mixer_out = dot(lax.all_gather(mixer_in, "tp", axis=1, tiled=True), out_weight).astype(jnp.bfloat16)
    resid = (stream.astype(jnp.float32) + mixer_out.astype(jnp.float32)).astype(jnp.bfloat16)
    normed_two = normalize(resid, moe_gain)
    core = lax.axis_index("tp")
    n2 = jnp.stack(
        [
            lax.dynamic_slice_in_dim(normed_two, core * HALF, HALF, 1),
            lax.dynamic_slice_in_dim(normed_two, (1 - core) * HALF, HALF, 1),
        ]
    )
    result = moe(
        n2, resid, route_ids, route_weights, dense_scale.reshape(1, HALF),
        expert_gate, expert_up, expert_down, dense_gate, dense_up, dense_down,
    )
    return (result, new_state, new_conv)


def solution(mesh):
    in_specs = (
        P("ep", "tp"), P("ep", None, "tp"), P("ep", "tp"), P(), P(None, "tp"), P(None, "tp"), P(None, "tp"),
        P("tp", None, None), P("tp", None, None), P("tp"), P(None, "tp"), P(), P("ep", None), P("ep", None),
        P("ep", None, "tp"), P("ep", None, "tp"), P("ep", None, "tp"), P(None, "tp"), P(None, "tp"),
        P(None, "tp"), P("tp"),
    )
    out_specs = (P("ep", "tp"), P("ep", "tp"), P("ep", None, "tp"))
    return jax.shard_map(per_device, mesh=mesh, in_specs=in_specs, out_specs=out_specs, check_vma=False)
```

```python
import jax
import jax.numpy as jnp
from jax import lax
from jax.experimental import pallas as pl
from jax.experimental.pallas import tpu as pltpu
from jax.sharding import PartitionSpec as P

BF = jnp.bfloat16
F32 = jnp.float32
MESH = pl.DeviceIdType.MESH

ROWS = 64
META = 8
BLOCK = ROWS + META
CUT = 40
HALF = 1024
LANES = ((0, 384), (384, 384), (768, 256))
ORDERS = ((0, 1, 2), (1, 2, 0), (2, 0, 1))
STRIDE = (16, 4, 1)
N_SEM = 320


ALL = slice(None)


def arranged(order, i, j):
    return (j, i) if order == 2 else (i, j)


def canonical(order, d, i):
    if order == 0:
        return (i, ALL, d)
    if order == 1:
        return (d, i, ALL)
    return (ALL, d, i)


def pair(h):
    return pl.ds(2 * h, 2)


def power_of_two(exponent):
    value = jnp.ones(exponent.shape, F32)
    for bit in range(6):
        value = value * jnp.where((exponent >> bit) & 1 == 1, F32(2.0 ** (2**bit)), F32(1.0))
    return value


def dot(a, b):
    return jnp.dot(a, b, preferred_element_type=F32)


def dot_t(a, b):
    return lax.dot_general(a, b, (((0,), (0,)), ((), ())), preferred_element_type=F32)


def layer_kernel(
    stream, ids_ref, wts_ref, mix_gain, moe_gain, taps, decay, scale_ref, conv_hbm, state_hbm, rmap_hbm, imap_hbm,
    wb, wg, wo, eg, eu, ed, dg, du, dd,
    rest, resid_out, branch_out, kept_out, driven_out,
    w_b, w_g, w_o, w_eg, w_eu, w_ed, w_dg, w_du, w_dd, conv_in, state_in, w_r, w_i, st, mi, r2, n2,
    ag0, ag1, ag2, cm0, cm1, cm2, ce0, ce1, ce2, fm0, fm1, fm2, fe0, fe1, fe2,
    xm, xe0, xe1, xe2, xx, hid, ym, yx, ye0, ye1, ye2,
    rm0, rm1, rm2, re0, re1, re2, gm0, gm1, gm2, ge0, ge1, ge2,
    pt0, pt1, pt2, sb0, sb1, sb2, rb0, rb1, rb2,
    pick_m, pick_e, comb_m, comb_e, dh, dense,
    ss, rs, ws,
):
    ag, cm, ce, fm, fe = (ag0, ag1, ag2), (cm0, cm1, cm2), (ce0, ce1, ce2), (fm0, fm1, fm2), (fe0, fe1, fe2)
    xe, ye, rm, re = (xe0, xe1, xe2), (ye0, ye1, ye2), (rm0, rm1, rm2), (re0, re1, re2)
    gm, ge, pt, sb, rb = (gm0, gm1, gm2), (ge0, ge1, ge2), (pt0, pt1, pt2), (sb0, sb1, sb2), (rb0, rb1, rb2)
    ep = lax.axis_index("ep")
    core = lax.axis_index("tp")
    coord = (ep // 16, (ep // 4) % 4, ep % 4)

    def along(axis, step):
        c = coord[axis]
        return ep + ((c + step) % 4 - c) * STRIDE[axis]

    next_dev = tuple((along(a, 1), core) for a in range(3))
    prev_dev = tuple((along(a, 3), core) for a in range(3))
    partner = (ep, 1 - core)

    barrier = pltpu.get_barrier_semaphore()
    for dev in (*next_dev, *prev_dev, partner):
        pl.semaphore_signal(barrier, inc=1, device_id=dev, device_id_type=MESH)

    loads = [0]

    def load(*copies):
        started = []
        for src, dst in copies:
            copy = pltpu.make_async_copy(src, dst, ws.at[loads[0]])
            loads[0] += 1
            copy.start()
            started.append(copy)
        return started

    def halves(src, dst, size):
        own = pl.multiple_of(core * size, size)
        other = pl.multiple_of((1 - core) * size, size)
        return (src.at[pl.ds(own, size)], dst.at[0]), (src.at[pl.ds(other, size)], dst.at[1])

    def landed(copies):
        for copy in copies:
            copy.wait()

    branch_load = load(*halves(wb, w_b, HALF))
    gate_load = load(
        (conv_hbm, conv_in), (rmap_hbm, w_r), (imap_hbm, w_i), (state_hbm, state_in), *halves(wg, w_g, HALF)
    )
    out_load = load(*halves(wo, w_o, HALF))

    used = [0]

    def remote(src, dst, dev):
        k = used[0]
        used[0] += 1
        return pltpu.make_async_remote_copy(
            src_ref=src, dst_ref=dst, send_sem=ss.at[k], recv_sem=rs.at[k], device_id=dev, device_id_type=MESH
        )

    sent = []

    def go(copy):
        copy.start()
        sent.append(copy)
        return copy

    lane = lax.broadcasted_iota(jnp.int32, (64, 128), 1)
    row = lax.broadcasted_iota(jnp.int32, (64, 128), 0)
    twice = (lane % 64 == row).astype(BF)
    ids_t = dot(ids_ref[...].astype(F32).astype(BF), twice)
    wts_t = dot(wts_ref[...].astype(BF), twice)
    experts = row.astype(F32)
    chosen = jnp.zeros((64, 128), F32)
    for k in range(6):
        chosen = chosen + jnp.where(ids_t[k : k + 1] == experts, F32(1.0), F32(0.0))
    earlier = (lane % 64 > row).astype(BF)
    rank = dot(chosen[:, :64].astype(BF), earlier)
    code = (rank + 32.0) * power_of_two(row)
    codes = [
        jnp.sum(jnp.where(ids_t[k : k + 1] == experts, code, F32(0.0)), axis=0, keepdims=True) for k in range(6)
    ]
    zeros2 = jnp.zeros((2, 128), F32)
    code8 = jnp.concatenate([*codes, zeros2], axis=0).astype(BF)
    wts8 = jnp.concatenate([wts_t, zeros2], axis=0).astype(BF)
    for o, (l0, w) in enumerate(LANES):
        ag[o][0, 0, ROWS:BLOCK, 0:128] = code8
        ag[o][0, 0, ROWS:BLOCK, 128:256] = wts8
        if w > 256:
            ag[o][0, 0, ROWS:BLOCK, 256:w] = jnp.zeros((META, w - 256), BF)
    for h in range(2):
        for o in range(3):
            comb_m[o, h] = jnp.zeros((512, 512), BF)
    for b in range(2):
        pick_m[b] = jnp.zeros((512, 512), BF)

    pl.semaphore_wait(barrier, 7)

    own_lanes = pl.ds(pl.multiple_of(core * HALF, HALF), HALF)
    other_lanes = pl.ds(pl.multiple_of((1 - core) * HALF, HALF), HALF)
    stream_copy = go(remote(stream, st, partner))
    shift = -decay[...]
    rate = -8.0 * (jnp.maximum(shift, 0.0) + jnp.log1p(jnp.exp(-jnp.abs(shift))))
    stream_copy.wait_recv()

    def normed(own_ref, other_ref, gain):
        a, b = own_ref.astype(F32), other_ref.astype(F32)
        total = jnp.sum(a, axis=1, keepdims=True) + jnp.sum(b, axis=1, keepdims=True)
        square = jnp.sum(a * a, axis=1, keepdims=True) + jnp.sum(b * b, axis=1, keepdims=True)
        mean = total * (1.0 / 2048)
        inv = lax.rsqrt(square * (1.0 / 2048) - mean * mean + 1e-05)
        return (
            ((a - mean) * inv * gain[:, own_lanes]).astype(BF),
            ((b - mean) * inv * gain[:, other_lanes]).astype(BF),
        )

    n_own, n_other = normed(stream[...], st[...], mix_gain)
    landed(branch_load)
    branch = (dot(n_own, w_b[0]) + dot(n_other, w_b[1])).astype(BF)
    branch_out[...] = branch
    landed(gate_load)
    late_load = load(*halves(dg, w_dg, HALF), *halves(du, w_du, HALF), *halves(dd, w_dd, 256))
    gate_pre = (dot(n_own, w_g[0]) + dot(n_other, w_g[1])).astype(BF)
    mixed = branch.astype(F32) * taps[3:4]
    for k in range(3):
        mixed = mixed + conv_in[k].astype(F32) * taps[k : k + 1]
    conv_out = mixed.astype(BF)
    for b in range(8):
        at = slice(128 * b, 128 * b + 128)
        piece = conv_out[:, at]
        recur_gate = jax.nn.sigmoid(dot(piece, w_r[b]))
        input_gate = jax.nn.sigmoid(dot(piece, w_i[b]))
        log_decay = recur_gate * rate[:, at]
        decayed = jnp.exp(log_decay)
        gap = jnp.tanh(-log_decay) * (1.0 + decayed * decayed)
        driven = jnp.sqrt(gap) * (input_gate * piece.astype(F32))
        kept = decayed * state_in[:, at]
        kept_out[:, at] = kept
        driven_out[:, at] = driven
        mi[0, :, at] = (jax.nn.gelu(gate_pre[:, at].astype(F32)) * (kept + driven)).astype(BF)
    mixer_copy = go(remote(mi.at[0], mi.at[1], partner))
    landed(out_load)
    expert_load = load(
        *halves(eg.at[0], w_eg, HALF), *halves(eu.at[0], w_eu, HALF), *halves(ed.at[0], w_ed, 256)
    )
    partial = dot(mi[0], w_o[0])
    mixer_copy.wait_recv()
    mixer_out = (partial + dot(mi[1], w_o[1])).astype(BF)
    r2[0] = (stream[...].astype(F32) + mixer_out.astype(F32)).astype(BF)
    resid_copy = go(remote(r2.at[0], r2.at[1], partner))
    resid_out[...] = r2[0]
    resid_copy.wait_recv()
    n_own, n_other = normed(r2[0], r2[1], moe_gain)
    n2[0] = n_own
    n2[1] = n_other
    for o, (l0, w) in enumerate(LANES):
        ag[o][0, 0, 0:ROWS, :] = n_own[:, l0 : l0 + w]

    def block(o, i, j, part=None):
        return ag[o].at[i, j] if part is None else ag[o].at[i, j, part]

    top, low = pl.ds(0, CUT), pl.ds(CUT, BLOCK - CUT)
    t1, t2, u1, u2 = {}, {}, {}, {}
    for o in range(3):
        a1 = ORDERS[o][0]
        t1[o] = (
            go(remote(block(o, 0, 0), block(o, 3, 0), next_dev[a1])),
            go(remote(block(o, 0, 0), block(o, 1, 0), prev_dev[a1])),
        )

    def spread(o, i):
        a2 = ORDERS[o][1]
        u1[o, i] = (
            go(remote(block(o, i, 0), block(o, i, 3), next_dev[a2])),
            go(remote(block(o, i, 0), block(o, i, 1), prev_dev[a2])),
        )

    def relay(o, i):
        a2 = ORDERS[o][1]
        u1[o, i][0].wait_recv()
        u1[o, i][1].wait_recv()
        u2[o, i] = (
            go(remote(block(o, i, 3, top), block(o, i, 2, top), next_dev[a2])),
            go(remote(block(o, i, 1, low), block(o, i, 2, low), prev_dev[a2])),
        )

    def relayed(o, i):
        u2[o, i][0].wait_recv()
        u2[o, i][1].wait_recv()

    for o in range(3):
        spread(o, 0)

    landed(late_load)
    d_gate = dot(n_own, w_dg[0]) + dot(n_other, w_dg[1])
    d_up = dot(n_own, w_du[0]) + dot(n_other, w_du[1])
    dh[0] = (jax.nn.silu(d_gate) * d_up).astype(BF)
    dh_copy = go(remote(dh.at[0], dh.at[1], partner))

    for o in range(3):
        a1 = ORDERS[o][0]
        t1[o][0].wait_recv()
        t1[o][1].wait_recv()
        t2[o] = (
            go(remote(block(o, 3, 0, top), block(o, 2, 0, top), next_dev[a1])),
            go(remote(block(o, 1, 0, low), block(o, 2, 0, low), prev_dev[a1])),
        )
    for o in range(3):
        spread(o, 1)
        spread(o, 3)
    for o in range(3):
        relay(o, 0)
    for o in range(3):
        t2[o][0].wait_recv()
        t2[o][1].wait_recv()
        spread(o, 2)
    for o in range(3):
        relay(o, 1)
    for o in range(3):
        relay(o, 3)
    for o in range(3):
        relay(o, 2)
    dh_copy.wait_recv()
    dense[...] = (dot(dh[0], w_dd[0]) + dot(dh[1], w_dd[1])).astype(BF).astype(F32)

    lane128 = lax.broadcasted_iota(jnp.int32, (16, 128), 1)
    rank16 = lax.broadcasted_iota(jnp.int32, (16, 128), 0).astype(F32) + 32.0
    lane512 = lax.broadcasted_iota(jnp.int32, (16, 512), 1)
    row512 = lax.broadcasted_iota(jnp.int32, (16, 512), 0)
    extra_rank = (row512 % 2).astype(F32) + 48.0
    extra_own = lane512 // 64 == row512 // 2
    first_half = lax.broadcasted_iota(jnp.int32, (8, 128), 1) < 64
    arrived = {}

    def pick(o, h, buf):
        l0, w = LANES[o]
        a3 = ORDERS[o][2]
        code, weight = [], []
        for p in range(4):
            i, j = 2 * h + p // 2, (2 * p) % 4
            for into, at in ((code, 0), (weight, 128)):
                a = ag[o][i, j, ROWS:BLOCK, at : at + 128].astype(F32)
                b = ag[o][i, j + 1, ROWS:BLOCK, at : at + 128].astype(F32)
                into.append(jnp.where(first_half, a, b))
        code = jnp.concatenate(code, axis=1)
        weight = jnp.concatenate(weight, axis=1)
        for d in range(4):
            scale = power_of_two(jnp.full((8, 512), along(a3, d), jnp.int32))
            mine = (code >= 32.0 * scale) & (code < 64.0 * scale)
            ranks = jnp.sum(jnp.where(mine, code, F32(0.0)), axis=0, keepdims=True)
            weights = jnp.sum(jnp.where(mine, weight, F32(0.0)), axis=0, keepdims=True)
            one = scale[0:1, 0:128]
            for s in range(8):
                lo = 128 * (s // 2)
                hit = (ranks[:, lo : lo + 128] == rank16 * one) & ((lane128 // 64) == s % 2)
                at = 128 * d + 16 * s
                pick_m[buf, at : at + 16, lo : lo + 128] = jnp.where(hit, F32(1.0), F32(0.0)).astype(BF)
                back_at = 128 * d + 16 * ((s % 4) * 2 + s // 4) if o == 2 else at
                comb_m[o, h, back_at : back_at + 16, lo : lo + 128] = jnp.where(
                    hit, weights[:, lo : lo + 128], F32(0.0)
                ).astype(BF)
            hit = (ranks == extra_rank * scale[0:1]) & extra_own
            pick_e[buf, 16 * d : 16 * d + 16] = jnp.where(hit, F32(1.0), F32(0.0)).astype(BF)
            comb_e[o, h, 16 * d : 16 * d + 16] = jnp.where(hit, weights, F32(0.0)).astype(BF)
        rows = ag[o][2 * h : 2 * h + 2, :, 0:ROWS, :].reshape(512, w)
        main = dot(pick_m[buf], rows).astype(BF)
        extra = dot(pick_e[buf], rows).astype(BF)
        for d in range(4):
            e = extra[16 * d : 16 * d + 16]
            for ii in range(2):
                at = 128 * d + 64 * ii
                m = main[at : at + 64].reshape(4, 16, w)
                if d == 0:
                    xm[(0, *canonical(o, 0, 2 * h + ii), ALL, pl.ds(l0, w))] = m
                else:
                    cm[o][(d - 1, *arranged(o, 2 * h + ii, ALL))] = m
            if d == 0:
                xe[o][0, 0, h] = e
            else:
                ce[o][d - 1, h] = e
        ahead, behind = next_dev[a3], prev_dev[a3]
        for ii in range(2):
            i = 2 * h + ii
            far = ahead if ii == 0 else behind
            arrived[o, 2, i] = (
                go(remote(cm[o].at[(1, *arranged(o, i, ALL))], fm[o].at[i], far)),
                go(remote(ce[o].at[1, h, pl.ds(8 * ii, 8)], fe[o].at[i], far)),
            )

    def direct(o, h):
        l0, w = LANES[o]
        a3 = ORDERS[o][2]
        ahead, behind = next_dev[a3], prev_dev[a3]
        into = lambda d: xm.at[(0, *canonical(o, d, pair(h)), ALL, pl.ds(l0, w))]
        arrived[o, 3, h] = (
            go(remote(cm[o].at[(0, *arranged(o, pair(h), ALL))], into(3), ahead)),
            go(remote(ce[o].at[0, h], xe[o].at[0, 3, h], ahead)),
        )
        arrived[o, 1, h] = (
            go(remote(cm[o].at[(2, *arranged(o, pair(h), ALL))], into(1), behind)),
            go(remote(ce[o].at[2, h], xe[o].at[0, 1, h], behind)),
        )

    def pass_on(o, h):
        l0, w = LANES[o]
        a3 = ORDERS[o][2]
        for ii in range(2):
            i = 2 * h + ii
            for copy in arrived[o, 2, i]:
                copy.wait_recv()
            far = next_dev[a3] if ii == 0 else prev_dev[a3]
            arrived[o, 4, i] = (
                go(remote(fm[o].at[i], xm.at[(0, *canonical(o, 2, i), ALL, pl.ds(l0, w))], far)),
                go(remote(fe[o].at[i], xe[o].at[0, 2, h, pl.ds(8 * ii, 8)], far)),
            )

    crossed = []

    def across(o, d):
        l0, w = LANES[o]
        at = (*canonical(o, d, ALL), ALL, pl.ds(l0, w))
        crossed.append(go(remote(xm.at[(0, *at)], xm.at[(1, *at)], partner)))
        crossed.append(go(remote(xe[o].at[0, d], xe[o].at[1, d], partner)))

    for o in range(3):
        relayed(o, 0)
        relayed(o, 1)
        pick(o, 0, 0)
    for o in range(3):
        direct(o, 0)
    for o in range(3):
        relayed(o, 2)
        relayed(o, 3)
        pick(o, 1, 1)
    for o in range(3):
        across(o, 0)
    for o in range(3):
        pass_on(o, 0)
    for o in range(3):
        direct(o, 1)
    for o in range(3):
        pass_on(o, 1)
    for o in range(3):
        for d in (3, 1):
            for h in range(2):
                for copy in arrived[o, d, h]:
                    copy.wait_recv()
            across(o, d)
    for o in range(3):
        for i in range(4):
            for copy in arrived[o, 4, i]:
                copy.wait_recv()
        across(o, 2)
    landed(expert_load)
    for copy in crossed:
        copy.wait_recv()

    r128 = lax.broadcasted_iota(jnp.int32, (128, 128), 0)
    c128 = lax.broadcasted_iota(jnp.int32, (128, 128), 1)
    dz, dy, dx, bit = r128 // 32, (r128 // 8) % 4, (r128 // 2) % 4, r128 % 2
    turn = {
        0: (c128 == (dx * 16 + dz * 4 + dy) * 2 + bit).astype(BF),
        2: (c128 == (dy * 16 + dx * 4 + dz) * 2 + bit).astype(BF),
    }
    for c in range(2):
        for o, (l0, w) in enumerate(LANES):
            rows = xe[o][c].reshape(128, w)
            xx[c, :, l0 : l0 + w] = rows if o == 1 else dot(turn[o], rows).astype(BF)

    hid_copies = []
    for b in range(5):
        if b < 4:
            x_own, x_other = xm[0, b].reshape(256, HALF), xm[1, b].reshape(256, HALF)
        else:
            x_own, x_other = xx[0], xx[1]
        at = slice(256 * b, 256 * b + x_own.shape[0])
        gate = dot(x_own, w_eg[0]) + dot(x_other, w_eg[1])
        up = dot(x_own, w_eu[0]) + dot(x_other, w_eu[1])
        hid[0, at] = (jax.nn.silu(gate) * up).astype(BF)
        span = pl.ds(256 * b, x_own.shape[0])
        hid_copies.append(go(remote(hid.at[0, span], hid.at[1, span], partner)))
    for b in range(5):
        hid_copies[b].wait_recv()
        size = 256 if b < 4 else 128
        at = slice(256 * b, 256 * b + size)
        y = (dot(hid[0, at], w_ed[0]) + dot(hid[1, at], w_ed[1])).astype(BF)
        if b < 4:
            ym[b] = y.reshape(4, 4, 16, HALF)
        else:
            yx[...] = y
    for o, (l0, w) in enumerate(LANES):
        rows = yx[:, l0 : l0 + w]
        rows = rows if o == 1 else dot_t(turn[o], rows).astype(BF)
        ye[o][...] = rows.reshape(4, 2, 16, w)

    back = {}

    def part(o, d, i):
        l0, w = LANES[o]
        return ym.at[(*canonical(o, d, i), ALL, pl.ds(l0, w))]

    def slots(o, h, d, ii=None):
        if ii is None:
            return rm[o].at[h, d]
        return rm[o].at[(h, d, *arranged(o, ii, ALL))]

    for h in (1, 0):
        for o in range(3):
            a3 = ORDERS[o][2]
            for ii in range(2):
                far = next_dev[a3] if ii == 0 else prev_dev[a3]
                i = 2 * h + ii
                back[o, 2, i] = (
                    go(remote(part(o, 2, i), gm[o].at[i], far)),
                    go(remote(ye[o].at[2, h, pl.ds(8 * ii, 8)], ge[o].at[i], far)),
                )

    def direct_back(h):
        for o in range(3):
            a3 = ORDERS[o][2]
            back[o, 3, h] = (
                go(remote(part(o, 1, pair(h)), slots(o, h, 3), next_dev[a3])),
                go(remote(ye[o].at[1, h], re[o].at[h, 3], next_dev[a3])),
            )
            back[o, 1, h] = (
                go(remote(part(o, 3, pair(h)), slots(o, h, 1), prev_dev[a3])),
                go(remote(ye[o].at[3, h], re[o].at[h, 1], prev_dev[a3])),
            )

    direct_back(1)
    for o, (l0, w) in enumerate(LANES):
        for h in range(2):
            rm[o][h, 0] = ym[(*canonical(o, 0, slice(2 * h, 2 * h + 2)), ALL, slice(l0, l0 + w))]
            re[o][h, 0] = ye[o][0, h]

    def pass_back(h):
        for o in range(3):
            a3 = ORDERS[o][2]
            for ii in range(2):
                i = 2 * h + ii
                for copy in back[o, 2, i]:
                    copy.wait_recv()
                far = next_dev[a3] if ii == 0 else prev_dev[a3]
                back[o, 4, i] = (
                    go(remote(gm[o].at[i], slots(o, h, 2, ii), far)),
                    go(remote(ge[o].at[i], re[o].at[h, 2, pl.ds(8 * ii, 8)], far)),
                )

    def combine(o, h):
        w = LANES[o][1]
        for key in ((o, 3, h), (o, 1, h), (o, 4, 2 * h), (o, 4, 2 * h + 1)):
            for copy in back[key]:
                copy.wait_recv()
        sums = dot_t(comb_m[o, h], rm[o][h].reshape(512, w)) + dot_t(comb_e[o, h], re[o][h].reshape(64, w))
        pt[o][2 * h : 2 * h + 2] = sums.reshape(2, 4, ROWS, w)

    up32, low32 = slice(0, 32), slice(32, 64)
    stage_a, stage_b = {}, {}

    def start_far(o, n, axis, src):
        sb[o][n, 0] = pt[o][src].astype(BF)
        stage_a[o, n] = (
            go(remote(sb[o].at[n, 0, pl.ds(0, 32)], rb[o].at[n, 0, pl.ds(0, 32)], prev_dev[axis])),
            go(remote(sb[o].at[n, 0, pl.ds(32, 32)], rb[o].at[n, 0, pl.ds(32, 32)], next_dev[axis])),
        )

    def start_near(o, n, axis, third, first):
        stage_a[o, n][0].wait_recv()
        stage_a[o, n][1].wait_recv()
        sb[o][n, 1, 0:32] = (pt[o][(*third, up32)] + rb[o][n, 0, 0:32].astype(F32)).astype(BF)
        sb[o][n, 1, 32:64] = pt[o][(*third, low32)].astype(BF)
        sb[o][n, 2, 0:32] = pt[o][(*first, up32)].astype(BF)
        sb[o][n, 2, 32:64] = (pt[o][(*first, low32)] + rb[o][n, 0, 32:64].astype(F32)).astype(BF)
        stage_b[o, n] = (
            go(remote(sb[o].at[n, 1], rb[o].at[n, 1], prev_dev[axis])),
            go(remote(sb[o].at[n, 2], rb[o].at[n, 2], next_dev[axis])),
        )

    def finish(o, n, home):
        stage_b[o, n][0].wait_recv()
        stage_b[o, n][1].wait_recv()
        pt[o][home] = pt[o][home] + rb[o][n, 1].astype(F32) + rb[o][n, 2].astype(F32)

    def far(i):
        for o in range(3):
            start_far(o, i, ORDERS[o][1], (i, 2))

    def near(i):
        for o in range(3):
            start_near(o, i, ORDERS[o][1], (i, 3), (i, 1))

    pass_back(1)
    pass_back(0)
    direct_back(0)
    for o in range(3):
        combine(o, 1)
        for i in (2, 3):
            start_far(o, i, ORDERS[o][1], (i, 2))
    near(2)
    near(3)
    for o in range(3):
        combine(o, 0)
        for i in (1, 0):
            start_far(o, i, ORDERS[o][1], (i, 2))
    for o in range(3):
        finish(o, 2, (2, 0))
        start_far(o, 4, ORDERS[o][0], (2, 0))
    near(1)
    near(0)
    for o in range(3):
        finish(o, 3, (3, 0))
        finish(o, 1, (1, 0))
        start_near(o, 4, ORDERS[o][0], (3, 0), (1, 0))
    for o in range(3):
        finish(o, 0, (0, 0))
    for o, (l0, w) in enumerate(LANES):
        finish(o, 4, (0, 0))
        at = slice(l0, l0 + w)
        rest[:, at] = pt[o][0, 0] + scale_ref[:, at] * dense[:, at]
    for copy in sent:
        copy.wait_send()


def layer(*args):
    vmem = pl.BlockSpec(memory_space=pltpu.VMEM)
    anyspace = pl.BlockSpec(memory_space=pl.ANY)
    widths = [w for _, w in LANES]
    per = lambda f, dt=BF: [pltpu.VMEM(f(w), dt) for w in widths]
    duo = lambda o: (4, 2) if o == 2 else (2, 4)
    scratch = [
        *[pltpu.VMEM((2, HALF, HALF), BF)] * 3,
        pltpu.VMEM((2, HALF, 256), BF), pltpu.VMEM((2, HALF, 256), BF), pltpu.VMEM((2, 256, HALF), BF),
        pltpu.VMEM((2, HALF, 256), BF), pltpu.VMEM((2, HALF, 256), BF), pltpu.VMEM((2, 256, HALF), BF),
        pltpu.VMEM((3, ROWS, HALF), BF), pltpu.VMEM((ROWS, HALF), F32),
        pltpu.VMEM((8, 128, 128), BF), pltpu.VMEM((8, 128, 128), BF),
        pltpu.VMEM((ROWS, HALF), BF),
        *[pltpu.VMEM((2, ROWS, HALF), BF)] * 3,
        *per(lambda w: (4, 4, BLOCK, w)),
        *per(lambda w: (3, 4, 4, 16, w)),
        *per(lambda w: (3, 2, 16, w)),
        *per(lambda w: (4, 4, 16, w)),
        *per(lambda w: (4, 8, w)),
        pltpu.VMEM((2, 4, 4, 4, 16, HALF), BF),
        *per(lambda w: (2, 4, 2, 16, w)),
        pltpu.VMEM((2, 128, HALF), BF),
        pltpu.VMEM((2, 1152, 256), BF),
        pltpu.VMEM((4, 4, 4, 16, HALF), BF),
        pltpu.VMEM((128, HALF), BF),
        *per(lambda w: (4, 2, 16, w)),
        *[pltpu.VMEM((2, 4, *duo(o), 16, w), BF) for o, w in enumerate(widths)],
        *per(lambda w: (2, 4, 16, w)),
        *per(lambda w: (4, 4, 16, w)),
        *per(lambda w: (4, 8, w)),
        *per(lambda w: (4, 4, ROWS, w), F32),
        *per(lambda w: (5, 3, ROWS, w)),
        *per(lambda w: (5, 3, ROWS, w)),
        pltpu.VMEM((2, 512, 512), BF), pltpu.VMEM((2, 64, 512), BF),
        pltpu.VMEM((3, 2, 512, 512), BF), pltpu.VMEM((3, 2, 64, 512), BF),
        pltpu.VMEM((2, ROWS, 256), BF), pltpu.VMEM((ROWS, HALF), F32),
        pltpu.SemaphoreType.DMA((N_SEM,)), pltpu.SemaphoreType.DMA((N_SEM,)), pltpu.SemaphoreType.DMA((24,)),
    ]
    wide = jax.ShapeDtypeStruct((ROWS, HALF), F32)
    short = jax.ShapeDtypeStruct((ROWS, HALF), BF)
    return pl.pallas_call(
        layer_kernel,
        out_shape=(wide, short, short, wide, wide),
        in_specs=[vmem] * 8 + [anyspace] * 13,
        out_specs=(vmem,) * 5,
        scratch_shapes=scratch,
        compiler_params=pltpu.CompilerParams(
            collective_id=0, has_side_effects=True, vmem_limit_bytes=58 * 1024 * 1024
        ),
        name="layer",
    )(*args)


def outputs_kernel(conv_hbm, rest, resid, branch, kept, driven, result, state, conv, r_buf, s_buf, c_buf, sems):
    old = pltpu.make_async_copy(conv_hbm.at[pl.ds(1, 2)], c_buf, sems.at[0])
    old.start()
    last = pltpu.make_async_copy(branch, conv.at[2], sems.at[1])
    last.start()
    s_buf[...] = kept[...] + driven[...]
    state_copy = pltpu.make_async_copy(s_buf, state, sems.at[2])
    state_copy.start()
    r_buf[...] = (resid[...].astype(F32) + rest[...]).astype(BF)
    result_copy = pltpu.make_async_copy(r_buf, result, sems.at[3])
    result_copy.start()
    old.wait()
    moved = pltpu.make_async_copy(c_buf, conv.at[pl.ds(0, 2)], sems.at[4])
    moved.start()
    for copy in (last, state_copy, result_copy, moved):
        copy.wait()


def outputs(*args):
    vmem = pl.BlockSpec(memory_space=pltpu.VMEM)
    anyspace = pl.BlockSpec(memory_space=pl.ANY)
    return pl.pallas_call(
        outputs_kernel,
        out_shape=(
            jax.ShapeDtypeStruct((ROWS, HALF), BF),
            jax.ShapeDtypeStruct((ROWS, HALF), F32),
            jax.ShapeDtypeStruct((3, ROWS, HALF), BF),
        ),
        in_specs=[anyspace] + [vmem] * 5,
        out_specs=(anyspace,) * 3,
        scratch_shapes=[
            pltpu.VMEM((ROWS, HALF), BF), pltpu.VMEM((ROWS, HALF), F32), pltpu.VMEM((2, ROWS, HALF), BF),
            pltpu.SemaphoreType.DMA((5,)),
        ],
        name="outputs",
    )(*args)


def per_device(
    stream, conv_state, recur_state, mix_gain, branch_weight, gate_weight, conv_taps, recur_map, input_map,
    decay_logit, out_weight, moe_gain, route_ids, route_weights, expert_gate, expert_up, expert_down,
    dense_gate, dense_up, dense_down, dense_scale,
):
    conv_turned = jnp.transpose(conv_state, (1, 0, 2))
    parts = layer(
        stream, route_ids.T, route_weights.T, mix_gain.reshape(1, -1), moe_gain.reshape(1, -1), conv_taps,
        decay_logit.reshape(1, -1), dense_scale.reshape(1, -1), conv_turned, recur_state,
        recur_map, input_map, branch_weight, gate_weight, out_weight,
        expert_gate, expert_up, expert_down, dense_gate, dense_up, dense_down,
    )
    result, new_state, new_conv = outputs(conv_turned, *parts)
    return (result, new_state, jnp.transpose(new_conv, (1, 0, 2)))


def solution(mesh):
    in_specs = (
        P("ep", "tp"), P("ep", None, "tp"), P("ep", "tp"), P(), P(None, "tp"), P(None, "tp"), P(None, "tp"),
        P("tp", None, None), P("tp", None, None), P("tp"), P(None, "tp"), P(), P("ep", None), P("ep", None),
        P("ep", None, "tp"), P("ep", None, "tp"), P("ep", None, "tp"), P(None, "tp"), P(None, "tp"),
        P(None, "tp"), P("tp"),
    )
    out_specs = (P("ep", "tp"), P("ep", "tp"), P("ep", None, "tp"))
    return jax.shard_map(per_device, mesh=mesh, in_specs=in_specs, out_specs=out_specs, check_vma=False)
```

```python
import jax
import jax.numpy as jnp
from jax import lax
from jax.experimental import pallas as pl
from jax.experimental.pallas import tpu as pltpu
from jax.sharding import PartitionSpec as P

BF = jnp.bfloat16
F32 = jnp.float32
MESH = pl.DeviceIdType.MESH
ALL = slice(None)

ROWS = 64
META = 8
BLOCK = ROWS + META
CUT = 40
HALF = 1024
LANES = ((0, 384), (384, 384), (768, 256))
ORDERS = ((0, 1, 2), (1, 2, 0), (2, 0, 1))
STRIDE = (16, 4, 1)
SLOTS = 48
NEAR = (0, 1, 3)


def canonical(order, d, i):
    if order == 0:
        return (i, ALL, d)
    if order == 1:
        return (d, i, ALL)
    return (ALL, d, i)


def power_of_two(exponent):
    value = jnp.ones(exponent.shape, F32)
    for bit in range(6):
        value = value * jnp.where((exponent >> bit) & 1 == 1, F32(2.0 ** (2**bit)), F32(1.0))
    return value


def dot(a, b):
    return jnp.dot(a, b, preferred_element_type=F32)


def dot_t(a, b):
    return lax.dot_general(a, b, (((0,), (0,)), ((), ())), preferred_element_type=F32)


def layer_kernel(
    stream_hbm, ids_hbm, wts_hbm, mix_gain_hbm, moe_gain_hbm, taps_hbm, decay_hbm, scale_hbm, conv_hbm, state_hbm,
    rmap_hbm, imap_hbm, wb, wg, wo, eg, eu, ed, dg, du, dd,
    rest, resid_out, branch_out, kept_out, driven_out,
    stream, ids_ref, wts_ref, mix_gain, moe_gain, taps, decay, scale_ref,
    w_b, w_g, w_o, w_eg, w_eu, w_ed, w_dg, w_du, w_dd, conv_in, state_in, w_r, w_i, st, mi, r2,
    ag0, ag1, ag2, cm0, cm1, cm2, ce0, ce1, ce2, fm0, fm1, fm2, fe0, fe1, fe2,
    xm, xe0, xe1, xe2, xx, hid, ym, yx, ye0, ye1, ye2,
    rm0, rm1, rm2, gm0, gm1, gm2, ge0, ge1, ge2,
    pt0, pt1, pt2, sb0, sb1, sb2, rb0, rb1, rb2,
    pick_m, comb_m, dh, dense,
    ss, rs, ws,
):
    ag, cm, ce, fm, fe = (ag0, ag1, ag2), (cm0, cm1, cm2), (ce0, ce1, ce2), (fm0, fm1, fm2), (fe0, fe1, fe2)
    xe, ye, rm = (xe0, xe1, xe2), (ye0, ye1, ye2), (rm0, rm1, rm2)
    gm, ge, pt, sb, rb = (gm0, gm1, gm2), (ge0, ge1, ge2), (pt0, pt1, pt2), (sb0, sb1, sb2), (rb0, rb1, rb2)
    ep = lax.axis_index("ep")
    core = lax.axis_index("tp")
    coord = (ep // 16, (ep // 4) % 4, ep % 4)

    def along(axis, step):
        c = coord[axis]
        return ep + ((c + step) % 4 - c) * STRIDE[axis]

    next_dev = tuple((along(a, 1), core) for a in range(3))
    prev_dev = tuple((along(a, 3), core) for a in range(3))
    partner = (ep, 1 - core)

    barrier = pltpu.get_barrier_semaphore()
    for dev in (*next_dev, *prev_dev, partner):
        pl.semaphore_signal(barrier, inc=1, device_id=dev, device_id_type=MESH)

    n_load = [0]

    def whole(src, dst):
        k = n_load[0]
        n_load[0] += 1
        copy = pltpu.make_async_copy(src, dst, ws.at[k])
        copy.start()
        return copy

    def halves(src, dst, size):
        k = n_load[0]
        n_load[0] += 1
        own = pl.multiple_of(core * size, size)
        other = pl.multiple_of((1 - core) * size, size)
        pltpu.make_async_copy(src.at[pl.ds(own, size)], dst.at[0], ws.at[k]).start()
        pltpu.make_async_copy(src.at[pl.ds(other, size)], dst.at[1], ws.at[k]).start()
        return pltpu.make_async_copy(dst, dst, ws.at[k])

    def landed(*copies):
        for copy in copies:
            copy.wait()

    ids_load, wts_load, stream_load = whole(ids_hbm, ids_ref), whole(wts_hbm, wts_ref), whole(stream_hbm, stream)
    small_load = (
        whole(mix_gain_hbm, mix_gain), whole(decay_hbm, decay), whole(taps_hbm, taps),
    )
    branch_load = halves(wb, w_b, HALF)
    gate_load = (
        whole(conv_hbm, conv_in), whole(rmap_hbm, w_r), whole(imap_hbm, w_i), whole(state_hbm, state_in),
        halves(wg, w_g, HALF),
    )
    out_load = halves(wo, w_o, HALF)
    norm_load = (whole(moe_gain_hbm, moe_gain), whole(scale_hbm, scale_ref))

    sends = []

    def go(tag, ref, dev, *pairs):
        k = len(sends)
        if k >= SLOTS:
            sends[k - SLOTS].wait()
        send_sem = ss.at[k % SLOTS]
        for src, dst in pairs:
            pltpu.make_async_remote_copy(
                src_ref=src, dst_ref=dst, send_sem=send_sem, recv_sem=rs.at[tag], device_id=dev, device_id_type=MESH
            ).start()
        sends.append(pltpu.make_async_copy(ref, ref, send_sem))

    def take(tag, ref):
        pltpu.make_async_copy(ref, ref, rs.at[tag]).wait()

    T1, T2, U1, U2 = 0, 3, 6, 18
    SUM_A, SUM_B = 0, 15
    FAR, DIRECT, PASSED = 30, 42, 54
    BACK_FAR, BACK = 66, 78
    CROSS, EXTRA, ROW = 90, 93, 94
    HIDDEN = 98

    for k in range(12):
        comb_m[k] = jnp.zeros((288, 256), BF)
    for b in range(3):
        pick_m[b] = jnp.zeros((288, 256), BF)
    lane = lax.broadcasted_iota(jnp.int32, (64, 128), 1)
    row = lax.broadcasted_iota(jnp.int32, (64, 128), 0)
    twice = (lane % 64 == row).astype(BF)
    landed(ids_load, wts_load)
    ids_t = dot(ids_ref[...].astype(F32).astype(BF), twice)
    wts_t = dot(wts_ref[...].astype(BF), twice)
    experts = row.astype(F32)
    chosen = jnp.zeros((64, 128), F32)
    for k in range(6):
        chosen = chosen + jnp.where(ids_t[k : k + 1] == experts, F32(1.0), F32(0.0))
    earlier = (lane % 64 > row).astype(BF)
    rank = dot(chosen[:, :64].astype(BF), earlier)
    code = (rank + 32.0) * power_of_two(row)
    codes = [
        jnp.sum(jnp.where(ids_t[k : k + 1] == experts, code, F32(0.0)), axis=0, keepdims=True) for k in range(6)
    ]
    zeros2 = jnp.zeros((2, 128), F32)
    code8 = jnp.concatenate([*codes, zeros2], axis=0).astype(BF)
    wts8 = jnp.concatenate([wts_t, zeros2], axis=0).astype(BF)
    for o, (l0, w) in enumerate(LANES):
        ag[o][0, 0, ROWS:BLOCK, 0:128] = code8
        ag[o][0, 0, ROWS:BLOCK, 128:256] = wts8
        if w > 256:
            ag[o][0, 0, ROWS:BLOCK, 256:w] = jnp.zeros((META, w - 256), BF)

    landed(stream_load)
    pl.semaphore_wait(barrier, 7)

    own_lanes = pl.ds(pl.multiple_of(core * HALF, HALF), HALF)
    other_lanes = pl.ds(pl.multiple_of((1 - core) * HALF, HALF), HALF)
    go(ROW, stream, partner, (stream, st))
    landed(*small_load)
    shift = -decay[...]
    rate = -8.0 * (jnp.maximum(shift, 0.0) + jnp.log1p(jnp.exp(-jnp.abs(shift))))
    take(ROW, st)

    def normed(own_ref, other_ref, gain):
        a, b = own_ref.astype(F32), other_ref.astype(F32)
        total = jnp.sum(a, axis=1, keepdims=True) + jnp.sum(b, axis=1, keepdims=True)
        square = jnp.sum(a * a, axis=1, keepdims=True) + jnp.sum(b * b, axis=1, keepdims=True)
        mean = total * (1.0 / 2048)
        inv = lax.rsqrt(square * (1.0 / 2048) - mean * mean + 1e-05)
        return (
            ((a - mean) * inv * gain[:, own_lanes]).astype(BF),
            ((b - mean) * inv * gain[:, other_lanes]).astype(BF),
        )

    n_own, n_other = normed(stream[...], st[...], mix_gain)
    landed(branch_load)
    branch = (dot(n_own, w_b[0]) + dot(n_other, w_b[1])).astype(BF)
    branch_out[...] = branch
    landed(*gate_load)
    dense_load = (halves(dg, w_dg, HALF), halves(du, w_du, HALF), halves(dd, w_dd, 256))
    gate_pre = (dot(n_own, w_g[0]) + dot(n_other, w_g[1])).astype(BF)
    mixed = branch.astype(F32) * taps[3:4]
    for k in range(3):
        mixed = mixed + conv_in[k].astype(F32) * taps[k : k + 1]
    conv_out = mixed.astype(BF)
    for b in range(8):
        at = slice(128 * b, 128 * b + 128)
        piece = conv_out[:, at]
        recur_gate = jax.nn.sigmoid(dot(piece, w_r[b]))
        input_gate = jax.nn.sigmoid(dot(piece, w_i[b]))
        log_decay = recur_gate * rate[:, at]
        decayed = jnp.exp(log_decay)
        gap = jnp.tanh(-log_decay) * (1.0 + decayed * decayed)
        driven = jnp.sqrt(gap) * (input_gate * piece.astype(F32))
        kept = decayed * state_in[:, at]
        kept_out[:, at] = kept
        driven_out[:, at] = driven
        mi[0, :, at] = (jax.nn.gelu(gate_pre[:, at].astype(F32)) * (kept + driven)).astype(BF)
    go(ROW + 1, mi.at[0], partner, (mi.at[0], mi.at[1]))
    landed(out_load)
    expert_load = (
        halves(eg.at[0], w_eg, HALF), halves(eu.at[0], w_eu, HALF), halves(ed.at[0], w_ed, 256),
    )
    partial = dot(mi[0], w_o[0])
    take(ROW + 1, mi.at[1])
    mixer_out = (partial + dot(mi[1], w_o[1])).astype(BF)
    r2[0] = (stream[...].astype(F32) + mixer_out.astype(F32)).astype(BF)
    go(ROW + 2, r2.at[0], partner, (r2.at[0], r2.at[1]))
    resid_out[...] = r2[0]
    landed(*norm_load)
    take(ROW + 2, r2.at[1])
    n_own, n_other = normed(r2[0], r2[1], moe_gain)
    for o, (l0, w) in enumerate(LANES):
        ag[o][0, 0, 0:ROWS, :] = n_own[:, l0 : l0 + w]

    def block(o, i, j, part=None):
        return ag[o].at[i, j] if part is None else ag[o].at[i, j, part]

    def one(o):
        return ag[o].at[0, 0]

    def two(o):
        return ag[o].at[0, pl.ds(0, 2)]

    def three(o):
        return ag[o].at[0, pl.ds(0, 3)]

    top, low = pl.ds(0, CUT), pl.ds(CUT, BLOCK - CUT)

    def spread(o, i):
        a2 = ORDERS[o][1]
        go(U1 + 4 * o + i, one(o), next_dev[a2], (block(o, i, 0), block(o, i, 3)))
        go(U1 + 4 * o + i, one(o), prev_dev[a2], (block(o, i, 0), block(o, i, 1)))

    def relay(o, i):
        a2 = ORDERS[o][1]
        take(U1 + 4 * o + i, two(o))
        tag = U2 + 4 * o + i
        go(tag, block(o, i, 2, top), next_dev[a2], (block(o, i, 3, top), block(o, i, 2, top)))
        go(tag, block(o, i, 2, low), prev_dev[a2], (block(o, i, 1, low), block(o, i, 2, low)))

    def relayed(o, i):
        take(U2 + 4 * o + i, one(o))

    for o in range(3):
        a1 = ORDERS[o][0]
        go(T1 + o, one(o), next_dev[a1], (block(o, 0, 0), block(o, 3, 0)))
        go(T1 + o, one(o), prev_dev[a1], (block(o, 0, 0), block(o, 1, 0)))
    for o in range(3):
        spread(o, 0)

    landed(*dense_load)
    d_gate = dot(n_own, w_dg[0]) + dot(n_other, w_dg[1])
    d_up = dot(n_own, w_du[0]) + dot(n_other, w_du[1])
    dh[0] = (jax.nn.silu(d_gate) * d_up).astype(BF)
    go(ROW + 3, dh.at[0], partner, (dh.at[0], dh.at[1]))

    for o in range(3):
        a1 = ORDERS[o][0]
        take(T1 + o, two(o))
        go(T2 + o, block(o, 2, 0, top), next_dev[a1], (block(o, 3, 0, top), block(o, 2, 0, top)))
        go(T2 + o, block(o, 2, 0, low), prev_dev[a1], (block(o, 1, 0, low), block(o, 2, 0, low)))
    for o in range(3):
        spread(o, 1)
        spread(o, 3)
    for o in range(3):
        relay(o, 0)
    take(ROW + 3, dh.at[1])
    dense[...] = (dot(dh[0], w_dd[0]) + dot(dh[1], w_dd[1])).astype(BF).astype(F32)
    for o in range(3):
        take(T2 + o, one(o))
        spread(o, 2)
    for o in range(3):
        relay(o, 1)
    for o in range(3):
        relay(o, 3)

    lane128 = lax.broadcasted_iota(jnp.int32, (16, 128), 1)
    rank16 = lax.broadcasted_iota(jnp.int32, (16, 128), 0).astype(F32) + 32.0
    lane256 = lax.broadcasted_iota(jnp.int32, (8, 256), 1)
    row256 = lax.broadcasted_iota(jnp.int32, (8, 256), 0)
    extra_rank = (row256 % 2).astype(F32) + 48.0
    extra_own = lane256 // 64 == row256 // 2
    first_half = lax.broadcasted_iota(jnp.int32, (8, 128), 1) < 64

    def eighth(i):
        return pl.ds(8 * (i % 2), 8)

    def pick(o, i):
        l0, w = LANES[o]
        a3 = ORDERS[o][2]
        code, weight = [], []
        for j in (0, 2):
            for into, at in ((code, 0), (weight, 128)):
                a = ag[o][i, j, ROWS:BLOCK, at : at + 128].astype(F32)
                b = ag[o][i, j + 1, ROWS:BLOCK, at : at + 128].astype(F32)
                into.append(jnp.where(first_half, a, b))
        code = jnp.concatenate(code, axis=1)
        weight = jnp.concatenate(weight, axis=1)
        for d in range(4):
            scale = power_of_two(jnp.full((8, 256), along(a3, d), jnp.int32))
            mine = (code >= 32.0 * scale) & (code < 64.0 * scale)
            ranks = jnp.sum(jnp.where(mine, code, F32(0.0)), axis=0, keepdims=True)
            weights = jnp.sum(jnp.where(mine, weight, F32(0.0)), axis=0, keepdims=True)
            unit = scale[0:1, 0:128]
            for j in range(4):
                lanes = slice(128 * (j // 2), 128 * (j // 2) + 128)
                hit = (ranks[:, lanes] == rank16 * unit) & ((lane128 // 64) == j % 2)
                at = slice(64 * d + 16 * j, 64 * d + 16 * j + 16)
                pick_m[o, at, lanes] = jnp.where(hit, F32(1.0), F32(0.0)).astype(BF)
                comb_m[4 * o + i, at, lanes] = jnp.where(hit, weights[:, lanes], F32(0.0)).astype(BF)
            hit = (ranks == extra_rank * scale[0:1]) & extra_own
            at = slice(256 + 8 * d, 256 + 8 * d + 8)
            pick_m[o, at] = jnp.where(hit, F32(1.0), F32(0.0)).astype(BF)
            comb_m[4 * o + i, at] = jnp.where(hit, weights, F32(0.0)).astype(BF)
        rows = dot(pick_m[o], ag[o][i, :, 0:ROWS, :].reshape(256, w)).astype(BF)
        for d in range(4):
            m = rows[64 * d : 64 * d + 64].reshape(4, 16, w)
            e = rows[256 + 8 * d : 256 + 8 * d + 8]
            if d == 0:
                xm[(0, *canonical(o, 0, i), ALL, pl.ds(l0, w))] = m
                xe[o][0, 0, i // 2, 8 * (i % 2) : 8 * (i % 2) + 8] = e
            else:
                cm[o][d - 1, i] = m
                ce[o][d - 1, i] = e
        far = next_dev[a3] if i % 2 == 0 else prev_dev[a3]
        go(FAR + 4 * o + i, one(o), far, (cm[o].at[1, i], fm[o].at[i]), (ce[o].at[1, i], fe[o].at[i]))

    def direct(o, i):
        l0, w = LANES[o]
        a3 = ORDERS[o][2]
        for source, d, dev in ((0, 3, next_dev[a3]), (2, 1, prev_dev[a3])):
            go(
                DIRECT + 4 * o + i, one(o), dev,
                (cm[o].at[source, i], xm.at[(0, *canonical(o, d, i), ALL, pl.ds(l0, w))]),
                (ce[o].at[source, i], xe[o].at[0, d, i // 2, eighth(i)]),
            )

    def pass_on(i):
        for o, (l0, w) in enumerate(LANES):
            a3 = ORDERS[o][2]
            take(FAR + 4 * o + i, one(o))
            go(
                PASSED + 4 * o + i, one(o), next_dev[a3] if i % 2 == 0 else prev_dev[a3],
                (fm[o].at[i], xm.at[(0, *canonical(o, 2, i), ALL, pl.ds(l0, w))]),
                (fe[o].at[i], xe[o].at[0, 2, i // 2, eighth(i)]),
            )

    def across(o, d, i):
        l0, w = LANES[o]
        at = (*canonical(o, d, i), ALL, pl.ds(l0, w))
        kind = 1 if d == 2 else 2 if i == 2 else 0
        go(CROSS + kind, fm[o].at[i], partner, (xm.at[(0, *at)], xm.at[(1, *at)]))

    def across_extra(o, d):
        go(EXTRA, xe[o].at[0, d], partner, (xe[o].at[0, d], xe[o].at[1, d]))

    def take_direct(i):
        for o in range(3):
            take(DIRECT + 4 * o + i, two(o))
            across(o, 3, i)
            across(o, 1, i)

    def take_passed(i):
        for o in range(3):
            take(PASSED + 4 * o + i, one(o))
            across(o, 2, i)

    def pick_unit(i):
        for o in range(3):
            pick(o, i)
        for o in range(3):
            direct(o, i)
        for o in range(3):
            across(o, 0, i)

    for o in range(3):
        relayed(o, 0)
    pick_unit(0)
    for o in range(3):
        relay(o, 2)
    for o in range(3):
        relayed(o, 1)
    pick_unit(1)
    for o in range(3):
        relayed(o, 3)
    pick_unit(3)
    for o in range(3):
        relayed(o, 2)
    for o in range(3):
        pick(o, 2)
    pass_on(0)
    for o in range(3):
        direct(o, 2)
        across(o, 0, 2)
    pass_on(1)
    pass_on(3)
    take_direct(0)
    take_direct(1)
    take_direct(3)
    pass_on(2)
    take_direct(2)
    for d in (0, 3, 1):
        for o in range(3):
            across_extra(o, d)
    take_passed(0)

    def gate_up(x_own, x_other, start, tag):
        size = x_own.shape[0]
        gate = dot(x_own, w_eg[0]) + dot(x_other, w_eg[1])
        up = dot(x_own, w_eu[0]) + dot(x_other, w_eu[1])
        hid[0, start : start + size] = (jax.nn.silu(gate) * up).astype(BF)
        span = pl.ds(start, size)
        go(HIDDEN + tag, hid.at[0, span], partner, (hid.at[0, span], hid.at[1, span]))

    def down(start, size, tag):
        take(HIDDEN + tag, hid.at[1, pl.ds(start, size)])
        at = slice(start, start + size)
        return (dot(hid[0, at], w_ed[0]) + dot(hid[1, at], w_ed[1])).astype(BF)

    def rows_of(c, groups):
        return jnp.concatenate([xm[(c, *g)].reshape(16 * n, HALF) for g, n in groups], axis=0)

    def put(y, groups):
        at = 0
        for g, n in groups:
            piece = y[at : at + 16 * n]
            ym[g] = piece.reshape(n, 16, HALF) if n > 1 else piece
            at += 16 * n

    early = [g for dz in NEAR for dy in NEAR for g in (((dz, dy, slice(0, 2)), 2), ((dz, dy, 3), 1))]
    mixed_rows = [g for dz in NEAR for g in (((dz, 2), 4), ((dz, 0, 2), 1), ((dz, 1, 2), 1), ((dz, 3, 2), 1))]
    landed(*expert_load)
    take(CROSS, xm.at[1, pl.ds(0, 3), pl.ds(0, 3)])
    gate_up(rows_of(0, early), rows_of(1, early), 0, 0)
    take_passed(1)
    take_passed(3)
    put(down(0, 432, 0), early)
    take_passed(2)
    for o in range(3):
        across_extra(o, 2)
    take(CROSS + 1, xm.at[1, 0])
    take(CROSS + 2, xm.at[1, pl.ds(0, 3), 0])
    gate_up(xm[0, 2].reshape(256, HALF), xm[1, 2].reshape(256, HALF), 432, 1)
    gate_up(rows_of(0, mixed_rows), rows_of(1, mixed_rows), 688, 2)
    take(EXTRA, xx.at[1])
    r128 = lax.broadcasted_iota(jnp.int32, (128, 128), 0)
    c128 = lax.broadcasted_iota(jnp.int32, (128, 128), 1)
    dz, dy, dx, bit = r128 // 32, (r128 // 8) % 4, (r128 // 2) % 4, r128 % 2
    turn = {
        0: (c128 == (dx * 16 + dz * 4 + dy) * 2 + bit).astype(BF),
        2: (c128 == (dy * 16 + dx * 4 + dz) * 2 + bit).astype(BF),
    }
    for c in range(2):
        for o, (l0, w) in enumerate(LANES):
            rows = xe[o][c].reshape(128, w)
            xx[c, :, l0 : l0 + w] = rows if o == 1 else dot(turn[o], rows).astype(BF)
    gate_up(xx[0], xx[1], 1024, 3)
    ym[2] = down(432, 256, 1).reshape(4, 4, 16, HALF)
    put(down(688, 336, 2), mixed_rows)
    yx[...] = down(1024, 128, 3)
    for o, (l0, w) in enumerate(LANES):
        rows = yx[:, l0 : l0 + w]
        rows = rows if o == 1 else dot_t(turn[o], rows).astype(BF)
        ye[o][...] = rows.reshape(4, 2, 16, w)

    def part(o, d, i):
        l0, w = LANES[o]
        return ym.at[(*canonical(o, d, i), ALL, pl.ds(l0, w))]

    def part_extra(o, d, i):
        return ye[o].at[d, i // 2, eighth(i)]

    def slot(o, d, i):
        return rm[o].at[i, pl.ds(4 * d, 4)]

    def slot_extra(o, d, i):
        return rm[o].at[i, 16 + d // 2, eighth(d)]

    def back_far(i):
        for o in range(3):
            a3 = ORDERS[o][2]
            go(
                BACK_FAR + 4 * o + i, one(o), next_dev[a3] if i % 2 == 0 else prev_dev[a3],
                (part(o, 2, i), gm[o].at[i]), (part_extra(o, 2, i), ge[o].at[i]),
            )

    def back_direct(i):
        for o in range(3):
            a3 = ORDERS[o][2]
            for d, dev in ((1, next_dev[a3]), (3, prev_dev[a3])):
                go(
                    BACK + 4 * o + i, one(o), dev,
                    (part(o, d, i), slot(o, 4 - d, i)), (part_extra(o, d, i), slot_extra(o, 4 - d, i)),
                )

    def pass_back(i):
        for o in range(3):
            a3 = ORDERS[o][2]
            take(BACK_FAR + 4 * o + i, one(o))
            go(
                BACK + 4 * o + i, one(o), next_dev[a3] if i % 2 == 0 else prev_dev[a3],
                (gm[o].at[i], slot(o, 2, i)), (ge[o].at[i], slot_extra(o, 2, i)),
            )

    def start_far(o, n, axis, src):
        sb[o][n, 0] = pt[o][src].astype(BF)
        half = sb[o].at[n, 0, pl.ds(0, 32)]
        go(SUM_A + 5 * o + n, half, prev_dev[axis], (half, rb[o].at[n, 0, pl.ds(0, 32)]))
        half = sb[o].at[n, 0, pl.ds(32, 32)]
        go(SUM_A + 5 * o + n, half, next_dev[axis], (half, rb[o].at[n, 0, pl.ds(32, 32)]))

    def start_near(o, n, axis, third, first):
        take(SUM_A + 5 * o + n, rb[o].at[n, 0])
        up32, low32 = slice(0, 32), slice(32, 64)
        sb[o][n, 1, 0:32] = (pt[o][(*third, up32)] + rb[o][n, 0, 0:32].astype(F32)).astype(BF)
        sb[o][n, 1, 32:64] = pt[o][(*third, low32)].astype(BF)
        sb[o][n, 2, 0:32] = pt[o][(*first, up32)].astype(BF)
        sb[o][n, 2, 32:64] = (pt[o][(*first, low32)] + rb[o][n, 0, 32:64].astype(F32)).astype(BF)
        go(SUM_B + 5 * o + n, sb[o].at[n, 1], prev_dev[axis], (sb[o].at[n, 1], rb[o].at[n, 1]))
        go(SUM_B + 5 * o + n, sb[o].at[n, 2], next_dev[axis], (sb[o].at[n, 2], rb[o].at[n, 2]))

    def finish(o, n, home):
        take(SUM_B + 5 * o + n, rb[o].at[n, pl.ds(1, 2)])
        pt[o][home] = pt[o][home] + rb[o][n, 1].astype(F32) + rb[o][n, 2].astype(F32)

    def combine(i):
        for o, (l0, w) in enumerate(LANES):
            take(BACK + 4 * o + i, three(o))
            sums = dot_t(comb_m[4 * o + i], rm[o][i].reshape(288, w))
            pt[o][i] = sums.reshape(4, ROWS, w)
            start_far(o, i, ORDERS[o][1], (i, 2))

    def near(i):
        for o in range(3):
            start_near(o, i, ORDERS[o][1], (i, 3), (i, 1))

    back_far(2)
    back_far(1)
    back_direct(2)
    back_far(3)
    back_direct(1)
    for o, (l0, w) in enumerate(LANES):
        for i in range(4):
            rm[o][i, 0:4] = ym[(*canonical(o, 0, i), ALL, slice(l0, l0 + w))]
            rm[o][i, 16, 0:8] = ye[o][0, i // 2, 8 * (i % 2) : 8 * (i % 2) + 8]
    pass_back(2)
    pass_back(1)
    back_direct(3)
    pass_back(3)
    back_far(0)
    back_direct(0)
    combine(2)
    combine(1)
    pass_back(0)
    combine(3)
    near(2)
    near(1)
    combine(0)
    near(3)
    for o in range(3):
        finish(o, 2, (2, 0))
        start_far(o, 4, ORDERS[o][0], (2, 0))
    near(0)
    for o in range(3):
        finish(o, 1, (1, 0))
    for o in range(3):
        finish(o, 3, (3, 0))
        start_near(o, 4, ORDERS[o][0], (3, 0), (1, 0))
    for o in range(3):
        finish(o, 0, (0, 0))
    for o, (l0, w) in enumerate(LANES):
        finish(o, 4, (0, 0))
        at = slice(l0, l0 + w)
        rest[:, at] = pt[o][0, 0] + scale_ref[:, at] * dense[:, at]
    for wait in sends[-SLOTS:]:
        wait.wait()


def layer(*args):
    vmem = pl.BlockSpec(memory_space=pltpu.VMEM)
    anyspace = pl.BlockSpec(memory_space=pl.ANY)
    widths = [w for _, w in LANES]
    per = lambda f, dt=BF: [pltpu.VMEM(f(w), dt) for w in widths]
    scratch = [
        pltpu.VMEM((ROWS, HALF), BF), pltpu.VMEM((6, ROWS), jnp.int32), pltpu.VMEM((6, ROWS), F32),
        pltpu.VMEM((1, 2048), F32), pltpu.VMEM((1, 2048), F32), pltpu.VMEM((4, HALF), F32),
        pltpu.VMEM((1, HALF), F32), pltpu.VMEM((1, HALF), F32),
        *[pltpu.VMEM((2, HALF, HALF), BF)] * 3,
        pltpu.VMEM((2, HALF, 256), BF), pltpu.VMEM((2, HALF, 256), BF), pltpu.VMEM((2, 256, HALF), BF),
        pltpu.VMEM((2, HALF, 256), BF), pltpu.VMEM((2, HALF, 256), BF), pltpu.VMEM((2, 256, HALF), BF),
        pltpu.VMEM((3, ROWS, HALF), BF), pltpu.VMEM((ROWS, HALF), F32),
        pltpu.VMEM((8, 128, 128), BF), pltpu.VMEM((8, 128, 128), BF),
        pltpu.VMEM((ROWS, HALF), BF), pltpu.VMEM((2, ROWS, HALF), BF), pltpu.VMEM((2, ROWS, HALF), BF),
        *per(lambda w: (4, 4, BLOCK, w)),
        *per(lambda w: (3, 4, 4, 16, w)),
        *per(lambda w: (3, 4, 8, w)),
        *per(lambda w: (4, 4, 16, w)),
        *per(lambda w: (4, 8, w)),
        pltpu.VMEM((2, 4, 4, 4, 16, HALF), BF),
        *per(lambda w: (2, 4, 2, 16, w)),
        pltpu.VMEM((2, 128, HALF), BF),
        pltpu.VMEM((2, 1152, 256), BF),
        pltpu.VMEM((4, 4, 4, 16, HALF), BF),
        pltpu.VMEM((128, HALF), BF),
        *per(lambda w: (4, 2, 16, w)),
        *per(lambda w: (4, 18, 16, w)),
        *per(lambda w: (4, 4, 16, w)),
        *per(lambda w: (4, 8, w)),
        *per(lambda w: (4, 4, ROWS, w), F32),
        *per(lambda w: (5, 3, ROWS, w)),
        *per(lambda w: (5, 3, ROWS, w)),
        pltpu.VMEM((3, 288, 256), BF), pltpu.VMEM((12, 288, 256), BF),
        pltpu.VMEM((2, ROWS, 256), BF), pltpu.VMEM((ROWS, HALF), F32),
        pltpu.SemaphoreType.DMA((SLOTS,)), pltpu.SemaphoreType.DMA((102,)), pltpu.SemaphoreType.DMA((22,)),
    ]
    wide = pltpu.VMEM((ROWS, HALF), F32)
    short = pltpu.VMEM((ROWS, HALF), BF)
    return pl.pallas_call(
        layer_kernel,
        out_shape=(wide, short, short, wide, wide),
        in_specs=[anyspace] * 21,
        out_specs=(vmem,) * 5,
        scratch_shapes=scratch,
        compiler_params=pltpu.CompilerParams(
            collective_id=0, has_side_effects=True, vmem_limit_bytes=56 * 1024 * 1024
        ),
        name="layer",
    )(*args)


def outputs_kernel(conv_hbm, rest, resid, branch, kept, driven, result, state, conv, r_buf, s_buf, c_buf, sems):
    old = pltpu.make_async_copy(conv_hbm.at[pl.ds(1, 2)], c_buf, sems.at[0])
    old.start()
    last = pltpu.make_async_copy(branch, conv.at[2], sems.at[1])
    last.start()
    s_buf[...] = kept[...] + driven[...]
    state_copy = pltpu.make_async_copy(s_buf, state, sems.at[2])
    state_copy.start()
    r_buf[...] = (resid[...].astype(F32) + rest[...]).astype(BF)
    result_copy = pltpu.make_async_copy(r_buf, result, sems.at[3])
    result_copy.start()
    old.wait()
    moved = pltpu.make_async_copy(c_buf, conv.at[pl.ds(0, 2)], sems.at[4])
    moved.start()
    for copy in (last, state_copy, result_copy, moved):
        copy.wait()


def outputs(*args):
    vmem = pl.BlockSpec(memory_space=pltpu.VMEM)
    anyspace = pl.BlockSpec(memory_space=pl.ANY)
    return pl.pallas_call(
        outputs_kernel,
        out_shape=(
            jax.ShapeDtypeStruct((ROWS, HALF), BF),
            jax.ShapeDtypeStruct((ROWS, HALF), F32),
            jax.ShapeDtypeStruct((3, ROWS, HALF), BF),
        ),
        in_specs=[anyspace] + [vmem] * 5,
        out_specs=(anyspace,) * 3,
        scratch_shapes=[
            pltpu.VMEM((ROWS, HALF), BF), pltpu.VMEM((ROWS, HALF), F32), pltpu.VMEM((2, ROWS, HALF), BF),
            pltpu.SemaphoreType.DMA((5,)),
        ],
        compiler_params=pltpu.CompilerParams(vmem_limit_bytes=4 * 1024 * 1024),
        name="outputs",
    )(*args)


def per_device(
    stream, conv_state, recur_state, mix_gain, branch_weight, gate_weight, conv_taps, recur_map, input_map,
    decay_logit, out_weight, moe_gain, route_ids, route_weights, expert_gate, expert_up, expert_down,
    dense_gate, dense_up, dense_down, dense_scale,
):
    conv_turned = jnp.transpose(conv_state, (1, 0, 2))
    parts = layer(
        stream, route_ids.T, route_weights.T, mix_gain.reshape(1, -1), moe_gain.reshape(1, -1), conv_taps,
        decay_logit.reshape(1, -1), dense_scale.reshape(1, -1), conv_turned, recur_state,
        recur_map, input_map, branch_weight, gate_weight, out_weight,
        expert_gate, expert_up, expert_down, dense_gate, dense_up, dense_down,
    )
    result, new_state, new_conv = outputs(conv_turned, *parts)
    return (result, new_state, jnp.transpose(new_conv, (1, 0, 2)))


def solution(mesh):
    in_specs = (
        P("ep", "tp"), P("ep", None, "tp"), P("ep", "tp"), P(), P(None, "tp"), P(None, "tp"), P(None, "tp"),
        P("tp", None, None), P("tp", None, None), P("tp"), P(None, "tp"), P(), P("ep", None), P("ep", None),
        P("ep", None, "tp"), P("ep", None, "tp"), P("ep", None, "tp"), P(None, "tp"), P(None, "tp"),
        P(None, "tp"), P("tp"),
    )
    out_specs = (P("ep", "tp"), P("ep", "tp"), P("ep", None, "tp"))
    return jax.shard_map(per_device, mesh=mesh, in_specs=in_specs, out_specs=out_specs, check_vma=False)
```
